512 devices in a mesh: fs: 128 (over z, x, core), tp: 4 (over y).
Axes of the slice: x: 4, y: 4, z: 16, core: 2. Of those that a mesh axis runs over, the one named last changes fastest.
Arguments:
- q_latent: bfloat16 [98304, 512], P('fs'), may hold values from -24 to 24
- q_grad: bfloat16 [98304, 3072], P('fs', 'tp'), may hold values from -6 to 6
- uq_master: float32 [512, 3072], P('fs', 'tp'), may hold values from -6 to 6
- uq_basis: bfloat16 [512, 256], P('fs'), may hold values from -4 to 4
- uq_first: float32 [256, 3072], P('fs', 'tp'), may hold values from -3 to 3
- uq_second: float32 [256, 3072], P('fs', 'tp'), may hold values from 0.1 to 1
- kv_latent: bfloat16 [98304, 512], P('fs'), may hold values from -24 to 24
- k_grad: bfloat16 [98304, 2048], P('fs', 'tp'), may hold values from -6 to 6
- uk_master: float32 [512, 2048], P('fs', 'tp'), may hold values from -6 to 6
- uk_basis: bfloat16 [512, 256], P('fs'), may hold values from -4 to 4
- uk_first: float32 [256, 2048], P('fs', 'tp'), may hold values from -3 to 3
- uk_second: float32 [256, 2048], P('fs', 'tp'), may hold values from 0.1 to 1
Outputs:
- uq_first_new: float32 [256, 3072], P('fs', 'tp')
- uq_second_new: float32 [256, 3072], P('fs', 'tp')
- uq_step: float32 [512, 3072], P('fs', 'tp')
- uq_copy: bfloat16 [512, 3072], P(None, 'tp')
- uk_first_new: float32 [256, 2048], P('fs', 'tp')
- uk_second_new: float32 [256, 2048], P('fs', 'tp')
- uk_step: float32 [512, 2048], P('fs', 'tp')
- uk_copy: bfloat16 [512, 2048], P(None, 'tp')
The draws below stay inside these ranges and needn't reach their ends.
All inputs are finite; a program needn't handle non-finite values.
Results may differ from the reference program's by a relative error of at most 0.0071.
Values may be sent and summed in bfloat16 or wider, within the bound.
A program may use at most 64 MiB of HBM per device.

```python
import math
import jax
import jax.numpy as jnp
from jax import lax

LATENT = 512
RANK = 256
TOKENS = 98304
QCOLS = 3072
KCOLS = 2048


def basis_draw(key):
    entries = jnp.clip(jax.random.normal(key, (LATENT, RANK), jnp.float32), -4.0, 4.0)
    column_scale = 10.0 ** (jnp.arange(RANK, dtype=jnp.float32) / (RANK - 1))
    return (entries * column_scale[None, :] / jnp.sqrt(LATENT * 1.0)).astype(jnp.bfloat16)


def draw_uq_basis(key, part):
    return basis_draw(jax.random.fold_in(key, 11))


def draw_uk_basis(key, part):
    return basis_draw(jax.random.fold_in(key, 12))


def strengthened(drawn, own_key, source, target, shards_of, factor):
    def block_of(axis_at):
        return (jnp.arange(drawn.shape[axis_at]) // (drawn.shape[axis_at] // shards_of)).reshape((-1,) + (1,) * (drawn.ndim - 1 - axis_at))

    near = jax.random.permutation(own_key, shards_of)[block_of(target)]
    far = (block_of(target) + shards_of // 2) % shards_of
    return jnp.where((block_of(source) == near) | (block_of(source) == far), factor * drawn, drawn)


def steps_of(own_key, shape, shards, least, largest):
    level = 1.0
    for axis_at, parts in shards:
        draws = jax.random.uniform(jax.random.fold_in(jax.random.fold_in(own_key, 6), axis_at), (parts,), jnp.float32, least / len(shards), largest / len(shards))
        level = level * jnp.repeat(jnp.exp(draws), shape[axis_at] // parts).reshape((-1,) + (1,) * (len(shape) - 1 - axis_at))
    return level


def centred(stream_key, extent, scale, bound, cuts=(), held_as=jnp.bfloat16):
    loudness = steps_of(stream_key, extent, cuts, -0.22, 0.18) if cuts else 1.0
    values = jax.random.normal(stream_key, extent, jnp.float32) * scale * loudness
    return jnp.minimum(jnp.maximum(values, -bound), bound).astype(held_as)


def bell_draw_with(stream_key, dims, scale, limit, shards, heavy, held_as=jnp.bfloat16):
    array = scale * jax.random.normal(stream_key, dims, jnp.float32)
    if shards:
        array = array * steps_of(stream_key, dims, shards, -0.22, 0.18)
    return jnp.clip(strengthened(array, jax.random.fold_in(stream_key, 3), *heavy), -limit, limit).astype(held_as)


def setup_inputs(seed: int = 0) -> dict:
    seeds = jax.random.split(jax.random.key(seed), 13)
    return {
        "q_latent": bell_draw_with(seeds[0], (TOKENS, LATENT), 1.0, 24.0, ((0, 128),), (0, 1, 128, 5.5)),
        "q_grad": centred(seeds[1], (TOKENS, QCOLS), 1.0, 6.0, ((0, 128), (1, 4))),
        "uq_master": centred(seeds[2], (LATENT, QCOLS), 1.0, 6.0, ((0, 128), (1, 4)), jnp.float32),
        "uq_basis": draw_uq_basis(jax.random.fold_in(seeds[12], 71), 0),
        "uq_first": centred(seeds[4], (RANK, QCOLS), 0.5, 3.0, ((0, 128), (1, 4)), jnp.float32),
        "uq_second": jnp.clip(jnp.exp(math.log(1.0) - 2.3025851 * jax.random.uniform(seeds[5], (RANK, QCOLS), jnp.float32) ** steps_of(seeds[5], (RANK, QCOLS), ((0, 128), (1, 4)), -0.2, 0.2)), 0.1, 1.0),
        "kv_latent": bell_draw_with(seeds[6], (TOKENS, LATENT), 1.0, 24.0, ((0, 128),), (0, 1, 128, 5.5)),
        "k_grad": centred(seeds[7], (TOKENS, KCOLS), 1.0, 6.0, ((0, 128), (1, 4))),
        "uk_master": centred(seeds[8], (LATENT, KCOLS), 1.0, 6.0, ((0, 128), (1, 4)), jnp.float32),
        "uk_basis": draw_uk_basis(jax.random.fold_in(seeds[12], 71), 0),
        "uk_first": centred(seeds[10], (RANK, KCOLS), 0.5, 3.0, ((0, 128), (1, 4)), jnp.float32),
        "uk_second": jnp.clip(jnp.exp(math.log(1.0) - 2.3025851 * jax.random.uniform(seeds[11], (RANK, KCOLS), jnp.float32) ** steps_of(seeds[11], (RANK, KCOLS), ((0, 128), (1, 4)), -0.2, 0.2)), 0.1, 1.0),
    }


first_decay = 0.8
second_decay = 0.9
step_size = 0.5
mean_guard = 1e-06
root_guard = 1e-08

def moment_update(scaled, first_old, second_old):
    first_new = first_decay * first_old + (1.0 - first_decay) * scaled
    second_new = second_decay * second_old + (1.0 - second_decay) * scaled * scaled
    heading = (first_new / (jnp.sqrt(second_new) + root_guard)).astype(jnp.bfloat16)
    return (first_new, second_new, heading)

def reference(q_latent, q_grad, uq_master, uq_basis, uq_first, uq_second, kv_latent, k_grad, uk_master, uk_basis, uk_first, uk_second):
    q_sum = jnp.dot(q_latent.T, q_grad, preferred_element_type=jnp.float32)
    k_sum = jnp.dot(kv_latent.T, k_grad, preferred_element_type=jnp.float32)
    q_proj = jnp.dot(uq_basis.astype(jnp.float32).T, q_sum, precision=lax.Precision.HIGHEST)
    k_proj = jnp.dot(uk_basis.astype(jnp.float32).T, k_sum, precision=lax.Precision.HIGHEST)
    squares_sum = jnp.sum(q_proj * q_proj) + jnp.sum(k_proj * k_proj)
    entry_count = q_proj.size + k_proj.size
    root_mean = jnp.sqrt(squares_sum / entry_count + mean_guard)
    uq_first_new, uq_second_new, q_dir = moment_update(q_proj / root_mean, uq_first, uq_second)
    uk_first_new, uk_second_new, k_dir = moment_update(k_proj / root_mean, uk_first, uk_second)
    uq_step = jnp.dot(uq_basis, q_dir, preferred_element_type=jnp.float32)
    uk_step = jnp.dot(uk_basis, k_dir, preferred_element_type=jnp.float32)
    uq_copy = (uq_master - step_size * uq_step).astype(jnp.bfloat16)
    uk_copy = (uk_master - step_size * uk_step).astype(jnp.bfloat16)
    return (uq_first_new, uq_second_new, uq_step, uq_copy, uk_first_new, uk_second_new, uk_step, uk_copy)
```

```python
import functools

import jax
import jax.numpy as jnp
from jax import lax
from jax.experimental import pallas as pl
from jax.experimental.pallas import tpu as pltpu
from jax.sharding import Mesh
from jax.sharding import PartitionSpec as P

AXES = ("z", "x", "c", "t")
FS = ("z", "x", "c")
MESH = pl.DeviceIdType.MESH
f32 = jnp.float32
bf16 = jnp.bfloat16

first_decay = 0.8
second_decay = 0.9
step_size = 0.5
mean_guard = 1e-06
root_guard = 1e-08


def log2(n):
    return n.bit_length() - 1


def part(v, low, size):
    return lax.shift_right_logical(v, low) & (size - 1)


def moved(rows, sizes):
    nz, nx, nc = sizes
    n = nz * nx * nc * rows
    lr, lz, lx, lc = log2(rows), log2(nz), log2(nx), log2(nc)
    nat = lax.broadcasted_iota(jnp.int32, (n, n), 0)
    got = lax.broadcasted_iota(jnp.int32, (n, n), 1)
    r = part(got, 0, rows)
    z = part(got, lr, nz)
    x = part(got, lr + lz, nx)
    c = part(got, lr + lz + lx, nc)
    want = ((z * nx + x) * nc + c) * rows + r
    return jnp.where(nat == want, 1.0, 0.0).astype(bf16)


def mul(a, b):
    return jnp.dot(a, b, preferred_element_type=f32)


def mul_t(a, b):
    return lax.dot_general(a, b, (((0,), (0,)), ((), ())), preferred_element_type=f32)


def kernel(sizes, widths, count, *refs):
    nz, nx, nc, nt = sizes
    qw, kw = widths
    (
        ql, qg, qm, qb, qf, qs, kl, kg, km, kb, kf, ks,
        qf_out, qs_out, qstep_out, qcopy_out, kf_out, ks_out, kstep_out, kcopy_out,
        ql_v, qg_v, kl_v, kg_v,
        bz, mo, mz, bslab, mslab, tokens, bnat, bperm, mnat, bwide, mwide, mold,
        prf, prs, rc, xs, rx, zf, zs, rz, ag, agf, sp, sz, hs,
        load_sem, zsend, zrecv, psend, precv, xsend, xrecv, csend, crecv,
    ) = refs
    w = qw + kw
    rank = qb.shape[1]
    z, x, c, t = (lax.axis_index(a) for a in AXES)
    other = 1 - c

    loads = [
        pltpu.make_async_copy(src, dst, load_sem.at[k])
        for k, (src, dst) in enumerate(((ql, ql_v), (qg, qg_v), (kl, kl_v), (kg, kg_v)))
    ]
    for load in loads:
        load.start()

    barrier = pltpu.get_barrier_semaphore()
    plane = nx * nc * nt
    mine = (x * nc + c) * nt + t

    def far(i):
        h = (i + 1) // 2
        return lax.rem(z + nz // 2 + h * (2 * lax.rem(i, 2) - 1) + nz, nz)

    def plane_peer(i):
        p = lax.rem(mine + i, plane)
        return (z, p // (nc * nt), lax.rem(p // nt, nc), lax.rem(p, nt)), p

    @pl.loop(0, nz - 1)
    def _(i):
        pl.semaphore_signal(barrier, inc=1, device_id=(far(i), x, c, t), device_id_type=MESH)

    @pl.loop(1, plane)
    def _(i):
        pl.semaphore_signal(barrier, inc=1, device_id=plane_peer(i)[0], device_id_type=MESH)

    bz[z, :, :rank] = qb[...]
    bz[z, :, rank:] = kb[...]
    mo[z, 0:2, :qw] = qf[...].astype(bf16)
    mo[z, 0:2, qw:] = kf[...].astype(bf16)
    mo[z, 2:4, :qw] = qs[...].astype(bf16)
    mo[z, 2:4, qw:] = ks[...].astype(bf16)
    mz[z, :, :qw] = qm[...].astype(bf16)
    mz[z, :, qw:] = km[...].astype(bf16)
    pl.semaphore_wait(barrier, nz - 1 + plane - 1)

    def z_copy(stage, src, dst, peer, slot):
        return pltpu.make_async_remote_copy(
            src_ref=src, dst_ref=dst,
            send_sem=zsend.at[stage, peer], recv_sem=zrecv.at[stage, slot],
            device_id=(peer, x, c, t), device_id_type=MESH,
        )

    def z_spread(stage, buf):
        @pl.loop(0, nz - 1)
        def _(i):
            z_copy(stage, buf.at[z], buf.at[z], far(i), z).start()

    def z_arrived(stage, buf):
        @pl.loop(0, nz - 1)
        def _(i):
            p = far(i)
            z_copy(stage, buf.at[p], buf.at[p], p, p).wait_recv()

    def z_left(stage, buf):
        @pl.loop(0, nz - 1)
        def _(i):
            p = far(i)
            z_copy(stage, buf.at[p], buf.at[p], p, p).wait_send()

    def x_copy(stage, src, dst, dx):
        p = lax.rem(x + dx, nx)
        return pltpu.make_async_remote_copy(
            src_ref=src, dst_ref=dst,
            send_sem=xsend.at[stage, dx], recv_sem=xrecv.at[stage, nx - dx],
            device_id=(z, p, c, t), device_id_type=MESH,
        )

    def x_from(stage, buf, dx):
        pltpu.make_async_remote_copy(
            src_ref=buf, dst_ref=buf,
            send_sem=xsend.at[stage, dx], recv_sem=xrecv.at[stage, dx],
            device_id=(z, lax.rem(x + dx, nx), c, t), device_id_type=MESH,
        ).wait_recv()

    def c_copy(stage, k, src, dst):
        return pltpu.make_async_remote_copy(
            src_ref=src, dst_ref=dst,
            send_sem=csend.at[stage, k], recv_sem=crecv.at[stage, k],
            device_id=(z, x, other, t), device_id_type=MESH,
        )

    def x_spread(stage, slabs):
        for dx in X_ORDER[nx]:
            x_copy(stage, slabs.at[c, x], slabs.at[c, x], dx).start()
        c_copy(stage, 0, slabs.at[c, x], slabs.at[c, x]).start()

    def x_onward(stage, slabs):
        for dx in X_ORDER[nx][::-1]:
            p = lax.rem(x + dx, nx)
            x_from(stage, slabs.at[c, p], dx)
            c_copy(stage, dx, slabs.at[c, p], slabs.at[c, p]).start()

    def x_arrived(stage, slabs):
        for dx in range(nx):
            p = lax.rem(x + dx, nx)
            c_copy(stage, dx, slabs.at[other, p], slabs.at[other, p]).wait_recv()

    def x_left(stage, slabs):
        for dx in range(1, nx):
            x_copy(stage, slabs.at[c, x], slabs.at[c, x], dx).wait_send()
        for dx in range(nx):
            p = lax.rem(x + dx, nx)
            c_copy(stage, dx, slabs.at[c, p], slabs.at[c, p]).wait_send()

    z_spread(0, bz)
    z_spread(1, mo)
    z_spread(2, mz)

    for load in loads[:2]:
        load.wait()
    tokens[:, :qw] = mul_t(ql_v[...], qg_v[...])
    for load in loads[2:]:
        load.wait()
    tokens[:, qw:] = mul_t(kl_v[...], kg_v[...])

    z_arrived(0, bz)
    lr = bz.shape[1]
    for k in range(nz):
        bwide[lr * k : lr * (k + 1), :] = bz[k].astype(f32)
    bslab[c, x] = bwide[...].astype(bf16)
    x_spread(0, bslab)
    by_latent = moved(lr, (nz, nx, nc))
    by_rank = moved(2, (nz, nx, nc))
    x_onward(0, bslab)
    x_arrived(0, bslab)
    latent = by_latent.shape[0]
    bnat[...] = mul(by_latent, bslab[...].reshape(latent, 2 * rank)).astype(bf16)
    bperm[:, :rank] = mul(bnat[:, :rank], by_rank).astype(bf16)
    bperm[:, rank:] = mul(bnat[:, rank:], by_rank).astype(bf16)

    def project(columns, basis):
        s = tokens[:, columns]
        high = s.astype(bf16)
        low = (s - high.astype(f32)).astype(bf16)
        got = mul_t(basis, high) + mul_t(basis, low)
        got = got.reshape(nc, nx, rank // (nc * nx), got.shape[1])
        prf[:, :, :, columns] = got
        prs[:, :, :, columns] = got.astype(bf16)

    project(slice(0, qw), bperm[:, :rank])
    project(slice(qw, w), bperm[:, rank:])

    order = X_ORDER[nx] + (0,)
    for dx in order:
        p = lax.rem(x + dx, nx)
        c_copy(1, dx, prs.at[other, p], rc.at[p]).start()
    for dx in order:
        p = lax.rem(x + dx, nx)
        c_copy(1, dx, rc.at[p], rc.at[p]).wait_recv()
        both = prf[c, p] + rc[p].astype(f32)
        if dx:
            xs[p] = both.astype(bf16)
            x_copy(1, xs.at[p], rx.at[x], dx).start()
        else:
            total = both

    z_arrived(2, mz)
    for k in range(nz):
        mwide[lr * k : lr * (k + 1), :] = mz[k].astype(f32)
    mslab[c, x] = mwide[...].astype(bf16)
    z_arrived(1, mo)
    for k in range(nz):
        mold[0, 2 * k : 2 * k + 2, :] = mo[k, 0:2].astype(f32)
        mold[1, 2 * k : 2 * k + 2, :] = mo[k, 2:4].astype(f32)
    x_spread(2, mslab)

    for dx in range(1, nx):
        p = lax.rem(x + dx, nx)
        x_from(1, rx.at[p], dx)
        total = total + rx[p].astype(f32)
    for k in range(nz):
        zf[k] = total[2 * k : 2 * k + 2]
        zs[k] = total[2 * k : 2 * k + 2].astype(bf16)
    rz[z] = jnp.zeros_like(rz[0])

    @pl.loop(0, nz - 1)
    def _(i):
        p = far(i)
        z_copy(3, zs.at[p], rz.at[z], p, z).start()

    x_onward(2, mslab)
    x_arrived(2, mslab)
    mnat[...] = mul(by_latent, mslab[...].reshape(latent, w))

    z_arrived(3, rz)
    proj = zf[z]
    for k in range(nz):
        proj = proj + rz[k].astype(f32)

    ag[z] = proj.astype(bf16)
    square = jnp.sum(proj * proj)
    sp[mine] = jnp.full((1, 128), square, f32)
    z_spread(4, ag)

    def p_copy(src, dst, peer, there, here):
        return pltpu.make_async_remote_copy(
            src_ref=src, dst_ref=dst,
            send_sem=psend.at[there], recv_sem=precv.at[here],
            device_id=peer, device_id_type=MESH,
        )

    @pl.loop(1, plane)
    def _(i):
        peer, p = plane_peer(i)
        p_copy(sp.at[mine], sp.at[mine], peer, p, mine).start()

    @pl.loop(1, plane)
    def _(i):
        peer, p = plane_peer(i)
        p_copy(sp.at[p], sp.at[p], peer, p, p).wait_recv()

    sz[z] = jnp.sum(sp[...], axis=0)
    z_spread(5, sz)
    z_arrived(4, ag)
    for k in range(nz):
        agf[2 * k : 2 * k + 2, :] = ag[k].astype(f32)
    z_arrived(5, sz)
    mean = jnp.sum(sz[...], axis=0)[:, 0:1] / count + mean_guard
    root_mean = jnp.sqrt(mean)

    def moments(scaled, first_old, second_old):
        first = first_decay * first_old + (1.0 - first_decay) * scaled
        second = second_decay * second_old + (1.0 - second_decay) * scaled * scaled
        return first, second

    first, second = moments(agf[...] / root_mean, mold[0], mold[1])
    hs[c, x] = (first / (jnp.sqrt(second) + root_guard)).astype(bf16)
    x_spread(3, hs)

    scaled = proj / root_mean
    first, second = moments(scaled[:, :qw], qf[...], qs[...])
    qf_out[...] = first
    qs_out[...] = second
    first, second = moments(scaled[:, qw:], kf[...], ks[...])
    kf_out[...] = first
    ks_out[...] = second
    own_q = mul(qb[...], by_rank).astype(bf16)
    own_k = mul(kb[...], by_rank).astype(bf16)

    x_onward(3, hs)
    x_arrived(3, hs)
    heading = hs[...].reshape(rank, w)
    qcopy_out[...] = (mnat[:, :qw] - step_size * mul(bperm[:, :rank], heading[:, :qw])).astype(bf16)
    kcopy_out[...] = (mnat[:, qw:] - step_size * mul(bperm[:, rank:], heading[:, qw:])).astype(bf16)
    qstep_out[...] = mul(own_q, heading[:, :qw])
    kstep_out[...] = mul(own_k, heading[:, qw:])

    for stage, buf in enumerate((bz, mo, mz, rz, ag, sz)):
        z_left(stage, buf)

    @pl.loop(1, plane)
    def _(i):
        peer, p = plane_peer(i)
        p_copy(sp.at[p], sp.at[p], peer, p, p).wait_send()

    x_left(0, bslab)
    x_left(2, mslab)
    x_left(3, hs)
    for dx in range(1, nx):
        p = lax.rem(x + dx, nx)
        x_copy(1, xs.at[p], rx.at[x], dx).wait_send()
    for dx in range(nx):
        p = lax.rem(x + dx, nx)
        c_copy(1, dx, prs.at[other, p], rc.at[p]).wait_send()


X_ORDER = {2: (1,), 4: (2, 1, 3)}


def body(sizes, *args):
    nz, nx, nc, nt = sizes
    ql, qg, qm, qb, qf, qs, kl, kg, km, kb, kf, ks = args
    qw, kw = qg.shape[1], kg.shape[1]
    w = qw + kw
    fs = nz * nx * nc
    lr, rank = qb.shape
    latent = lr * fs
    rows = rank // (nc * nx)
    count = float(rank * w * nt)
    plane = nx * nc * nt
    vmem = pl.BlockSpec(memory_space=pltpu.VMEM)
    anywhere = pl.BlockSpec(memory_space=pl.ANY)
    shape = jax.ShapeDtypeStruct
    return pl.pallas_call(
        functools.partial(kernel, sizes, (qw, kw), count),
        out_shape=(
            shape(qf.shape, f32), shape(qs.shape, f32), shape(qm.shape, f32), shape((latent, qw), bf16),
            shape(kf.shape, f32), shape(ks.shape, f32), shape(km.shape, f32), shape((latent, kw), bf16),
        ),
        in_specs=[anywhere, anywhere, vmem, vmem, vmem, vmem] * 2,
        out_specs=[vmem] * 8,
        scratch_shapes=[
            pltpu.VMEM(ql.shape, bf16), pltpu.VMEM(qg.shape, bf16),
            pltpu.VMEM(kl.shape, bf16), pltpu.VMEM(kg.shape, bf16),
            pltpu.VMEM((nz, lr, 2 * rank), bf16),
            pltpu.VMEM((nz, 4, w), bf16),
            pltpu.VMEM((nz, lr, w), bf16),
            pltpu.VMEM((nc, nx, nz * lr, 2 * rank), bf16),
            pltpu.VMEM((nc, nx, nz * lr, w), bf16),
            pltpu.VMEM((latent, w), f32),
            pltpu.VMEM((latent, 2 * rank), bf16),
            pltpu.VMEM((latent, 2 * rank), bf16),
            pltpu.VMEM((latent, w), f32),
            pltpu.VMEM((nz * lr, 2 * rank), f32),
            pltpu.VMEM((nz * lr, w), f32),
            pltpu.VMEM((2, rows, w), f32),
            pltpu.VMEM((nc, nx, rows, w), f32),
            pltpu.VMEM((nc, nx, rows, w), bf16),
            pltpu.VMEM((nx, rows, w), bf16),
            pltpu.VMEM((nx, rows, w), bf16),
            pltpu.VMEM((nx, rows, w), bf16),
            pltpu.VMEM((nz, 2, w), f32),
            pltpu.VMEM((nz, 2, w), bf16),
            pltpu.VMEM((nz, 2, w), bf16),
            pltpu.VMEM((nz, 2, w), bf16),
            pltpu.VMEM((rows, w), f32),
            pltpu.VMEM((plane, 1, 128), f32),
            pltpu.VMEM((nz, 1, 128), f32),
            pltpu.VMEM((nc, nx, rows, w), bf16),
            pltpu.SemaphoreType.DMA((4,)),
            pltpu.SemaphoreType.DMA((6, nz)), pltpu.SemaphoreType.DMA((6, nz)),
            pltpu.SemaphoreType.DMA((plane,)), pltpu.SemaphoreType.DMA((plane,)),
            pltpu.SemaphoreType.DMA((4, nx)), pltpu.SemaphoreType.DMA((4, nx)),
            pltpu.SemaphoreType.DMA((4, nx)), pltpu.SemaphoreType.DMA((4, nx)),
        ],
        compiler_params=pltpu.CompilerParams(
            collective_id=0, has_side_effects=True, vmem_limit_bytes=56 * 1024 * 1024
        ),
    )(*args)


def solution(mesh, chips=(16, 4, 2)):
    nt = mesh.shape["tp"]
    finer = Mesh(mesh.devices.reshape(*chips, nt), AXES)
    in_specs = (P(FS, None), P(FS, "t"), P(FS, "t"), P(FS, None), P(FS, "t"), P(FS, "t")) * 2
    out_specs = (P(FS, "t"), P(FS, "t"), P(FS, "t"), P(None, "t")) * 2
    return jax.shard_map(
        functools.partial(body, (*chips, nt)), mesh=finer, in_specs=in_specs, out_specs=out_specs, check_vma=False
    )
```

```python
import functools

import jax
import jax.numpy as jnp
from jax import lax
from jax.experimental import pallas as pl
from jax.experimental.pallas import tpu as pltpu
from jax.sharding import Mesh
from jax.sharding import PartitionSpec as P

AXES = ("z", "x", "c", "t")
FS = ("z", "x", "c")
MESH = pl.DeviceIdType.MESH
f32 = jnp.float32
bf16 = jnp.bfloat16

first_decay = 0.8
second_decay = 0.9
step_size = 0.5
mean_guard = 1e-06
root_guard = 1e-08


def log2(n):
    return n.bit_length() - 1


def part(v, low, size):
    return lax.shift_right_logical(v, low) & (size - 1)


def moved(rows, sizes):
    nz, nx, nc = sizes
    n = nz * nx * nc * rows
    lr, lz, lx, lc = log2(rows), log2(nz), log2(nx), log2(nc)
    nat = lax.broadcasted_iota(jnp.int32, (n, n), 0)
    got = lax.broadcasted_iota(jnp.int32, (n, n), 1)
    r = part(got, 0, rows)
    z = part(got, lr, nz)
    x = part(got, lr + lz, nx)
    c = part(got, lr + lz + lx, nc)
    want = ((z * nx + x) * nc + c) * rows + r
    return jnp.where(nat == want, 1.0, 0.0).astype(bf16)


def mul(a, b):
    return jnp.dot(a, b, preferred_element_type=f32)


def mul_t(a, b):
    return lax.dot_general(a, b, (((0,), (0,)), ((), ())), preferred_element_type=f32)


def kernel(sizes, widths, count, *refs):
    nz, nx, nc, nt = sizes
    qw, kw = widths
    (
        ql, qg, qm_h, qb, qf_h, qs_h, kl, kg, km_h, kb, kf_h, ks_h,
        hs, bperm, mnat, proj_out, mean_out,
        ql_v, qg_v, kl_v, kg_v, qm, qf, qs, km, kf, ks,
        bz, mo, mz, bslab, mslab, tokens, bnat, bwide, mwide, mold,
        prf, prs, rc, xs, rx, zf, zs, rz, ag, agf, sp, sz,
        load_sem, zsend, zrecv, psend, precv, xsend, xrecv, csend, crecv,
    ) = refs
    w = qw + kw
    rank = qb.shape[1]
    z, x, c, t = (lax.axis_index(a) for a in AXES)
    other = 1 - c

    loads = [
        pltpu.make_async_copy(src, dst, load_sem.at[k])
        for k, (src, dst) in enumerate((
            (ql, ql_v), (qg, qg_v), (kl, kl_v), (kg, kg_v),
            (qb, bz.at[z, :, :rank]), (kb, bz.at[z, :, rank:]),
            (qf_h, qf), (qs_h, qs), (kf_h, kf), (ks_h, ks), (qm_h, qm), (km_h, km),
        ))
    ]
    for load in loads[4:] + loads[:4]:
        load.start()

    barrier = pltpu.get_barrier_semaphore()
    plane = nx * nc * nt
    mine = (x * nc + c) * nt + t

    def far(i):
        h = (i + 1) // 2
        return lax.rem(z + nz // 2 + h * (2 * lax.rem(i, 2) - 1) + nz, nz)

    def plane_peer(i):
        p = lax.rem(mine + i, plane)
        return (z, p // (nc * nt), lax.rem(p // nt, nc), lax.rem(p, nt)), p

    @pl.loop(0, nz - 1)
    def _(i):
        pl.semaphore_signal(barrier, inc=1, device_id=(far(i), x, c, t), device_id_type=MESH)

    @pl.loop(1, plane)
    def _(i):
        pl.semaphore_signal(barrier, inc=1, device_id=plane_peer(i)[0], device_id_type=MESH)

    for load in loads[4:]:
        load.wait()
    mo[z, 0:2, :qw] = qf[...].astype(bf16)
    mo[z, 0:2, qw:] = kf[...].astype(bf16)
    mo[z, 2:4, :qw] = qs[...].astype(bf16)
    mo[z, 2:4, qw:] = ks[...].astype(bf16)
    mz[z, :, :qw] = qm[...].astype(bf16)
    mz[z, :, qw:] = km[...].astype(bf16)
    pl.semaphore_wait(barrier, nz - 1 + plane - 1)

    def z_copy(stage, src, dst, peer, slot):
        return pltpu.make_async_remote_copy(
            src_ref=src, dst_ref=dst,
            send_sem=zsend.at[stage, peer], recv_sem=zrecv.at[stage, slot],
            device_id=(peer, x, c, t), device_id_type=MESH,
        )

    def z_spread(stage, buf):
        @pl.loop(0, nz - 1)
        def _(i):
            z_copy(stage, buf.at[z], buf.at[z], far(i), z).start()

    def z_arrived(stage, buf):
        @pl.loop(0, nz - 1)
        def _(i):
            p = far(i)
            z_copy(stage, buf.at[p], buf.at[p], p, p).wait_recv()

    def z_left(stage, buf):
        @pl.loop(0, nz - 1)
        def _(i):
            p = far(i)
            z_copy(stage, buf.at[p], buf.at[p], p, p).wait_send()

    def x_copy(stage, src, dst, dx):
        p = lax.rem(x + dx, nx)
        return pltpu.make_async_remote_copy(
            src_ref=src, dst_ref=dst,
            send_sem=xsend.at[stage, dx], recv_sem=xrecv.at[stage, nx - dx],
            device_id=(z, p, c, t), device_id_type=MESH,
        )

    def x_from(stage, buf, dx):
        pltpu.make_async_remote_copy(
            src_ref=buf, dst_ref=buf,
            send_sem=xsend.at[stage, dx], recv_sem=xrecv.at[stage, dx],
            device_id=(z, lax.rem(x + dx, nx), c, t), device_id_type=MESH,
        ).wait_recv()

    def c_copy(stage, k, src, dst):
        return pltpu.make_async_remote_copy(
            src_ref=src, dst_ref=dst,
            send_sem=csend.at[stage, k], recv_sem=crecv.at[stage, k],
            device_id=(z, x, other, t), device_id_type=MESH,
        )

    def x_spread(stage, slabs):
        for dx in X_ORDER[nx]:
            x_copy(stage, slabs.at[c, x], slabs.at[c, x], dx).start()
        c_copy(stage, 0, slabs.at[c, x], slabs.at[c, x]).start()

    def x_onward(stage, slabs):
        for dx in X_ORDER[nx][::-1]:
            p = lax.rem(x + dx, nx)
            x_from(stage, slabs.at[c, p], dx)
            c_copy(stage, dx, slabs.at[c, p], slabs.at[c, p]).start()

    def x_arrived(stage, slabs):
        for dx in range(nx):
            p = lax.rem(x + dx, nx)
            c_copy(stage, dx, slabs.at[other, p], slabs.at[other, p]).wait_recv()

    def x_left(stage, slabs):
        for dx in range(1, nx):
            x_copy(stage, slabs.at[c, x], slabs.at[c, x], dx).wait_send()
        for dx in range(nx):
            p = lax.rem(x + dx, nx)
            c_copy(stage, dx, slabs.at[c, p], slabs.at[c, p]).wait_send()

    z_spread(0, bz)
    z_spread(1, mo)
    z_spread(2, mz)

    for load in loads[:2]:
        load.wait()
    tokens[:, :qw] = mul_t(ql_v[...], qg_v[...])
    for load in loads[2:4]:
        load.wait()
    tokens[:, qw:] = mul_t(kl_v[...], kg_v[...])

    z_arrived(0, bz)
    lr = bz.shape[1]
    for k in range(nz):
        bwide[lr * k : lr * (k + 1), :] = bz[k].astype(f32)
    bslab[c, x] = bwide[...].astype(bf16)
    x_spread(0, bslab)
    by_latent = moved(lr, (nz, nx, nc))
    by_rank = moved(2, (nz, nx, nc))
    x_onward(0, bslab)
    x_arrived(0, bslab)
    latent = by_latent.shape[0]
    bnat[...] = mul(by_latent, bslab[...].reshape(latent, 2 * rank)).astype(bf16)
    bperm[:, :rank] = mul(bnat[:, :rank], by_rank).astype(bf16)
    bperm[:, rank:] = mul(bnat[:, rank:], by_rank).astype(bf16)

    def project(columns, basis):
        s = tokens[:, columns]
        high = s.astype(bf16)
        low = (s - high.astype(f32)).astype(bf16)
        got = mul_t(basis, high) + mul_t(basis, low)
        got = got.reshape(nc, nx, rank // (nc * nx), got.shape[1])
        prf[:, :, :, columns] = got
        prs[:, :, :, columns] = got.astype(bf16)

    project(slice(0, qw), bperm[:, :rank])
    project(slice(qw, w), bperm[:, rank:])

    order = X_ORDER[nx] + (0,)
    for dx in order:
        p = lax.rem(x + dx, nx)
        c_copy(1, dx, prs.at[other, p], rc.at[p]).start()
    for dx in order:
        p = lax.rem(x + dx, nx)
        c_copy(1, dx, rc.at[p], rc.at[p]).wait_recv()
        both = prf[c, p] + rc[p].astype(f32)
        if dx:
            xs[p] = both.astype(bf16)
            x_copy(1, xs.at[p], rx.at[x], dx).start()
        else:
            total = both

    z_arrived(2, mz)
    for k in range(nz):
        mwide[lr * k : lr * (k + 1), :] = mz[k].astype(f32)
    mslab[c, x] = mwide[...].astype(bf16)
    z_arrived(1, mo)
    for k in range(nz):
        mold[0, 2 * k : 2 * k + 2, :] = mo[k, 0:2].astype(f32)
        mold[1, 2 * k : 2 * k + 2, :] = mo[k, 2:4].astype(f32)
    x_spread(2, mslab)

    for dx in range(1, nx):
        p = lax.rem(x + dx, nx)
        x_from(1, rx.at[p], dx)
        total = total + rx[p].astype(f32)
    for k in range(nz):
        zf[k] = total[2 * k : 2 * k + 2]
        zs[k] = total[2 * k : 2 * k + 2].astype(bf16)
    rz[z] = jnp.zeros_like(rz[0])

    @pl.loop(0, nz - 1)
    def _(i):
        p = far(i)
        z_copy(3, zs.at[p], rz.at[z], p, z).start()

    x_onward(2, mslab)
    x_arrived(2, mslab)
    mnat[...] = mul(by_latent, mslab[...].reshape(latent, w)).astype(bf16)

    z_arrived(3, rz)
    proj = zf[z]
    for k in range(nz):
        proj = proj + rz[k].astype(f32)

    ag[z] = proj.astype(bf16)
    square = jnp.sum(proj * proj)
    sp[mine] = jnp.full((1, 128), square, f32)
    z_spread(4, ag)

    def p_copy(src, dst, peer, there, here):
        return pltpu.make_async_remote_copy(
            src_ref=src, dst_ref=dst,
            send_sem=psend.at[there], recv_sem=precv.at[here],
            device_id=peer, device_id_type=MESH,
        )

    @pl.loop(1, plane)
    def _(i):
        peer, p = plane_peer(i)
        p_copy(sp.at[mine], sp.at[mine], peer, p, mine).start()

    @pl.loop(1, plane)
    def _(i):
        peer, p = plane_peer(i)
        p_copy(sp.at[p], sp.at[p], peer, p, p).wait_recv()

    sz[z] = jnp.sum(sp[...], axis=0)
    z_spread(5, sz)
    z_arrived(4, ag)
    for k in range(nz):
        agf[2 * k : 2 * k + 2, :] = ag[k].astype(f32)
    z_arrived(5, sz)
    mean = jnp.sum(sz[...], axis=0)[:, 0:1] / count + mean_guard
    root_mean = jnp.sqrt(mean)

    first, second = moments(agf[...] / root_mean, mold[0], mold[1])
    hs[c, x] = (first / (jnp.sqrt(second) + root_guard)).astype(bf16)
    x_spread(3, hs)

    proj_out[...] = proj
    mean_out[...] = jnp.broadcast_to(root_mean, mean_out.shape)
    x_onward(3, hs)
    x_arrived(3, hs)
    for stage, buf in enumerate((bz, mo, mz, rz, ag, sz)):
        z_left(stage, buf)

    @pl.loop(1, plane)
    def _(i):
        peer, p = plane_peer(i)
        p_copy(sp.at[p], sp.at[p], peer, p, p).wait_send()

    x_left(0, bslab)
    x_left(2, mslab)
    x_left(3, hs)
    for dx in range(1, nx):
        p = lax.rem(x + dx, nx)
        x_copy(1, xs.at[p], rx.at[x], dx).wait_send()
    for dx in range(nx):
        p = lax.rem(x + dx, nx)
        c_copy(1, dx, prs.at[other, p], rc.at[p]).wait_send()


def moments(scaled, first_old, second_old):
    first = first_decay * first_old + (1.0 - first_decay) * scaled
    second = second_decay * second_old + (1.0 - second_decay) * scaled * scaled
    return first, second


def finish(sizes, *refs):
    (
        heading, basis, master, proj, mean, qb, qf, qs, kb, kf, ks,
        qf_out, qs_out, qstep_out, qcopy_out, kf_out, ks_out, kstep_out, kcopy_out,
    ) = refs
    nz, nx, nc, nt = sizes
    rank = qb.shape[1]
    qw = qf.shape[1]
    by_rank = moved(2, (nz, nx, nc))
    scaled = proj[...] / mean[:, 0:1]
    qf_out[...], qs_out[...] = moments(scaled[:, :qw], qf[...], qs[...])
    kf_out[...], ks_out[...] = moments(scaled[:, qw:], kf[...], ks[...])
    own_q = mul(qb[...], by_rank).astype(bf16)
    own_k = mul(kb[...], by_rank).astype(bf16)
    q_dir = heading[:, :qw]
    k_dir = heading[:, qw:]
    qstep_out[...] = mul(own_q, q_dir)
    kstep_out[...] = mul(own_k, k_dir)
    q_step = mul(basis[:, :rank], q_dir)
    qcopy_out[...] = (master[:, :qw].astype(f32) - step_size * q_step).astype(bf16)
    k_step = mul(basis[:, rank:], k_dir)
    kcopy_out[...] = (master[:, qw:].astype(f32) - step_size * k_step).astype(bf16)


X_ORDER = {2: (1,), 4: (2, 1, 3)}


def body(sizes, *args):
    nz, nx, nc, nt = sizes
    args = [pltpu.with_memory_space_constraint(a, pltpu.HBM) for a in args]
    ql, qg, qm, qb, qf, qs, kl, kg, km, kb, kf, ks = args
    qw, kw = qg.shape[1], kg.shape[1]
    w = qw + kw
    fs = nz * nx * nc
    lr, rank = qb.shape
    latent = lr * fs
    rows = rank // (nc * nx)
    count = float(rank * w * nt)
    plane = nx * nc * nt
    vmem = pl.BlockSpec(memory_space=pltpu.VMEM)
    shape = jax.ShapeDtypeStruct
    hbm = pl.BlockSpec(memory_space=pltpu.HBM)
    heading, basis, master, proj, mean = pl.pallas_call(
        functools.partial(kernel, sizes, (qw, kw), count),
        out_shape=(
            shape((nc, nx, rows, w), bf16), shape((latent, 2 * rank), bf16), shape((latent, w), bf16),
            shape((2, w), f32), shape((1, 128), f32),
        ),
        in_specs=[hbm] * 12,
        out_specs=[vmem] * 5,
        scratch_shapes=[
            pltpu.VMEM(ql.shape, bf16), pltpu.VMEM(qg.shape, bf16),
            pltpu.VMEM(kl.shape, bf16), pltpu.VMEM(kg.shape, bf16),
            *(pltpu.VMEM(a.shape, f32) for a in (qm, qf, qs, km, kf, ks)),
            pltpu.VMEM((nz, lr, 2 * rank), bf16),
            pltpu.VMEM((nz, 4, w), bf16),
            pltpu.VMEM((nz, lr, w), bf16),
            pltpu.VMEM((nc, nx, nz * lr, 2 * rank), bf16),
            pltpu.VMEM((nc, nx, nz * lr, w), bf16),
            pltpu.VMEM((latent, w), f32),
            pltpu.VMEM((latent, 2 * rank), bf16),
            pltpu.VMEM((nz * lr, 2 * rank), f32),
            pltpu.VMEM((nz * lr, w), f32),
            pltpu.VMEM((2, rows, w), f32),
            pltpu.VMEM((nc, nx, rows, w), f32),
            pltpu.VMEM((nc, nx, rows, w), bf16),
            pltpu.VMEM((nx, rows, w), bf16),
            pltpu.VMEM((nx, rows, w), bf16),
            pltpu.VMEM((nx, rows, w), bf16),
            pltpu.VMEM((nz, 2, w), f32),
            pltpu.VMEM((nz, 2, w), bf16),
            pltpu.VMEM((nz, 2, w), bf16),
            pltpu.VMEM((nz, 2, w), bf16),
            pltpu.VMEM((rows, w), f32),
            pltpu.VMEM((plane, 1, 128), f32),
            pltpu.VMEM((nz, 1, 128), f32),
            pltpu.SemaphoreType.DMA((12,)),
            pltpu.SemaphoreType.DMA((6, nz)), pltpu.SemaphoreType.DMA((6, nz)),
            pltpu.SemaphoreType.DMA((plane,)), pltpu.SemaphoreType.DMA((plane,)),
            pltpu.SemaphoreType.DMA((4, nx)), pltpu.SemaphoreType.DMA((4, nx)),
            pltpu.SemaphoreType.DMA((4, nx)), pltpu.SemaphoreType.DMA((4, nx)),
        ],
        compiler_params=pltpu.CompilerParams(
            collective_id=0, has_side_effects=True, vmem_limit_bytes=28 * 1024 * 1024
        ),
    )(*args)
    return pl.pallas_call(
        functools.partial(finish, sizes),
        out_shape=(
            shape(qf.shape, f32), shape(qs.shape, f32), shape(qm.shape, f32), shape((latent, qw), bf16),
            shape(kf.shape, f32), shape(ks.shape, f32), shape(km.shape, f32), shape((latent, kw), bf16),
        ),
        in_specs=[vmem] * 11,
        out_specs=[vmem] * 8,
        compiler_params=pltpu.CompilerParams(vmem_limit_bytes=20 * 1024 * 1024),
    )(heading.reshape(rank, w), basis, master, proj, mean, qb, qf, qs, kb, kf, ks)


def solution(mesh, chips=(16, 4, 2)):
    nt = mesh.shape["tp"]
    finer = Mesh(mesh.devices.reshape(*chips, nt), AXES)
    in_specs = (P(FS, None), P(FS, "t"), P(FS, "t"), P(FS, None), P(FS, "t"), P(FS, "t")) * 2
    out_specs = (P(FS, "t"), P(FS, "t"), P(FS, "t"), P(None, "t")) * 2
    return jax.shard_map(
        functools.partial(body, (*chips, nt)), mesh=finer, in_specs=in_specs, out_specs=out_specs, check_vma=False
    )
```

```python
import functools

import jax
import jax.numpy as jnp
from jax import lax
from jax.experimental import pallas as pl
from jax.experimental.pallas import tpu as pltpu
from jax.sharding import Mesh
from jax.sharding import PartitionSpec as P

AXES = ("z", "x", "c", "t")
FS = ("z", "x", "c")
MESH = pl.DeviceIdType.MESH
f32 = jnp.float32
bf16 = jnp.bfloat16

first_decay = 0.8
second_decay = 0.9
step_size = 0.5
mean_guard = 1e-06
root_guard = 1e-08


def log2(n):
    return n.bit_length() - 1


def part(v, low, size):
    return lax.shift_right_logical(v, low) & (size - 1)


def moved(rows, sizes, back=False):
    nz, nx, nc = sizes
    n = nz * nx * nc * rows
    lr, lz, lx, lc = log2(rows), log2(nz), log2(nx), log2(nc)
    nat = lax.broadcasted_iota(jnp.int32, (n, n), int(back))
    got = lax.broadcasted_iota(jnp.int32, (n, n), 1 - int(back))
    r = part(got, 0, rows)
    z = part(got, lr, nz)
    x = part(got, lr + lz, nx)
    c = part(got, lr + lz + lx, nc)
    want = ((z * nx + x) * nc + c) * rows + r
    return jnp.where(nat == want, 1.0, 0.0).astype(bf16)


def mul(a, b):
    return jnp.dot(a, b, preferred_element_type=f32)


def mul_by_t(a, b):
    return lax.dot_general(a, b, (((1,), (1,)), ((), ())), preferred_element_type=f32)


def mul_t(a, b):
    return lax.dot_general(a, b, (((0,), (0,)), ((), ())), preferred_element_type=f32)


def kernel(sizes, widths, count, *refs):
    nz, nx, nc, nt = sizes
    qw, kw = widths
    (
        ql, qg, qm_h, qb, qf_h, qs_h, kl, kg, km_h, kb, kf_h, ks_h,
        heads, ps, bnat, mnat, scale_out,
        ql_v, qg_v, kl_v, kg_v, qm, qf, qs, km, kf, ks,
        bz, mo, mz, bslab, oslab, mslab, tokens, rounded, wide, wider, mold,
        rc, xs, rx, hilo, pt, zs, rz, ag, sp, sz,
        load_sem, zsend, zrecv, psend, precv, xsend, xrecv, csend, crecv,
    ) = refs
    w = qw + kw
    rank = qb.shape[1]
    lr = bz.shape[1]
    latent = lr * nz * nx * nc
    share = w // (nc * nx)
    lanes = pt.shape[2]
    halves = rank // lanes
    pairs = share // nz // 2
    z, x, c, t = (lax.axis_index(a) for a in AXES)
    other = 1 - c

    loads = [
        pltpu.make_async_copy(src, dst, load_sem.at[k])
        for k, (src, dst) in enumerate((
            (ql, ql_v), (qg, qg_v), (kl, kl_v), (kg, kg_v),
            (qb, bz.at[z, :, :rank]), (kb, bz.at[z, :, rank:]),
            (qf_h, qf), (qs_h, qs), (kf_h, kf), (ks_h, ks), (qm_h, qm), (km_h, km),
        ))
    ]
    for load in loads:
        load.start()

    barrier = pltpu.get_barrier_semaphore()
    plane = nx * nc * nt
    mine = (x * nc + c) * nt + t

    def far(i):
        h = (i + 1) // 2
        return lax.rem(z + nz // 2 + h * (2 * lax.rem(i, 2) - 1) + nz, nz)

    def plane_peer(i):
        p = lax.rem(mine + i, plane)
        return (z, p // (nc * nt), lax.rem(p // nt, nc), lax.rem(p, nt)), p

    @pl.loop(0, nz - 1)
    def _(i):
        pl.semaphore_signal(barrier, inc=1, device_id=(far(i), x, c, t), device_id_type=MESH)

    @pl.loop(1, plane)
    def _(i):
        pl.semaphore_signal(barrier, inc=1, device_id=plane_peer(i)[0], device_id_type=MESH)

    def z_copy(stage, src, dst, peer, slot):
        return pltpu.make_async_remote_copy(
            src_ref=src, dst_ref=dst,
            send_sem=zsend.at[stage, peer], recv_sem=zrecv.at[stage, slot],
            device_id=(peer, x, c, t), device_id_type=MESH,
        )

    def z_spread(stage, buf):
        @pl.loop(0, nz - 1)
        def _(i):
            z_copy(stage, buf.at[z], buf.at[z], far(i), z).start()

    def z_arrived(stage, buf):
        @pl.loop(0, nz - 1)
        def _(i):
            p = far(i)
            z_copy(stage, buf.at[p], buf.at[p], p, p).wait_recv()

    def z_left(stage, buf):
        @pl.loop(0, nz - 1)
        def _(i):
            p = far(i)
            z_copy(stage, buf.at[p], buf.at[p], p, p).wait_send()

    def x_copy(stage, src, dst, dx):
        p = lax.rem(x + dx, nx)
        return pltpu.make_async_remote_copy(
            src_ref=src, dst_ref=dst,
            send_sem=xsend.at[stage, dx], recv_sem=xrecv.at[stage, nx - dx],
            device_id=(z, p, c, t), device_id_type=MESH,
        )

    def x_from(stage, buf, dx):
        pltpu.make_async_remote_copy(
            src_ref=buf, dst_ref=buf,
            send_sem=xsend.at[stage, dx], recv_sem=xrecv.at[stage, dx],
            device_id=(z, lax.rem(x + dx, nx), c, t), device_id_type=MESH,
        ).wait_recv()

    def c_copy(stage, k, src, dst):
        return pltpu.make_async_remote_copy(
            src_ref=src, dst_ref=dst,
            send_sem=csend.at[stage, k], recv_sem=crecv.at[stage, k],
            device_id=(z, x, other, t), device_id_type=MESH,
        )

    def x_spread(stage, slabs):
        for dx in X_ORDER[nx]:
            x_copy(stage, slabs.at[c, x], slabs.at[c, x], dx).start()
        c_copy(stage, 0, slabs.at[c, x], slabs.at[c, x]).start()

    def x_onward(stage, slabs):
        for dx in X_ORDER[nx][::-1]:
            p = lax.rem(x + dx, nx)
            x_from(stage, slabs.at[c, p], dx)
            c_copy(stage, dx, slabs.at[c, p], slabs.at[c, p]).start()

    def x_arrived(stage, slabs):
        for dx in range(nx):
            p = lax.rem(x + dx, nx)
            c_copy(stage, dx, slabs.at[other, p], slabs.at[other, p]).wait_recv()

    def x_left(stage, slabs):
        for dx in range(1, nx):
            x_copy(stage, slabs.at[c, x], slabs.at[c, x], dx).wait_send()
        for dx in range(nx):
            p = lax.rem(x + dx, nx)
            c_copy(stage, dx, slabs.at[c, p], slabs.at[c, p]).wait_send()

    def rows(core, p):
        return pl.ds(pl.multiple_of((core * nx + p) * share, share), share)

    for load in loads[:2]:
        load.wait()
    tokens[:qw] = mul_t(qg_v[...], ql_v[...])
    for load in loads[2:4]:
        load.wait()
    tokens[qw:] = mul_t(kg_v[...], kl_v[...])
    rounded[...] = tokens[...].astype(bf16)
    for load in loads[4:]:
        load.wait()
    mo[z, 0:2, :qw] = qf[...].astype(bf16)
    mo[z, 0:2, qw:] = kf[...].astype(bf16)
    mo[z, 2:4, :qw] = qs[...].astype(bf16)
    mo[z, 2:4, qw:] = ks[...].astype(bf16)
    mz[z, :, :qw] = qm[...].astype(bf16)
    mz[z, :, qw:] = km[...].astype(bf16)
    pl.semaphore_wait(barrier, nz - 1 + plane - 1)

    order = X_ORDER[nx] + (0,)
    z_spread(0, bz)
    for dx in order:
        p = lax.rem(x + dx, nx)
        c_copy(1, dx, rounded.at[rows(other, p)], rc.at[p]).start()
    z_spread(1, mo)
    z_spread(2, mz)
    for dx in order:
        p = lax.rem(x + dx, nx)
        c_copy(1, dx, rc.at[p], rc.at[p]).wait_recv()
        both = tokens[rows(c, p)] + rc[p].astype(f32)
        if dx:
            xs[p] = both.astype(bf16)
            x_copy(1, xs.at[p], rx.at[x], dx).start()
        else:
            tokens[rows(c, p)] = both
    by_latent = moved(lr, (nz, nx, nc))

    z_arrived(0, bz)
    for k in range(nz):
        wide[lr * k : lr * (k + 1), :] = bz[k].astype(f32)
    bslab[c, x] = wide[...].astype(bf16)
    x_spread(0, bslab)

    total = tokens[rows(c, x)]
    for dx in range(1, nx):
        p = lax.rem(x + dx, nx)
        x_from(1, rx.at[p], dx)
        total = total + rx[p].astype(f32)
    high = total.astype(bf16)
    low = (total - high.astype(f32)).astype(bf16)
    part_of = latent // nc
    turned_high = mul(high, by_latent).astype(bf16)
    turned_low = mul(low, by_latent).astype(bf16)
    for k in range(nc):
        hilo[k, :share] = turned_high[:, k * part_of : (k + 1) * part_of]
        hilo[k, share:] = turned_low[:, k * part_of : (k + 1) * part_of]

    x_onward(0, bslab)
    got = mul(hilo[c], bslab[c].reshape(part_of, 2 * rank))
    x_arrived(0, bslab)
    got = got + mul(hilo[other], bslab[other].reshape(part_of, 2 * rank))
    got = got[:share] + got[share:]
    column = (c * nx + x) * share + lax.broadcasted_iota(jnp.int32, (share, rank), 0)
    got = jnp.where(column < qw, got[:, :rank], got[:, rank:])
    for h in range(halves):
        pt[h] = got[:, h * lanes : (h + 1) * lanes]
    for k in range(nz):
        for h in range(halves):
            for j in range(pairs):
                first = 2 * (k * pairs + j)
                zs[k, h * pairs + j] = pt[h, first : first + 2].astype(bf16)

    @pl.loop(0, nz - 1)
    def _(i):
        p = far(i)
        z_copy(3, zs.at[p], rz.at[z], p, z).start()

    rz[z] = zs[z]

    z_arrived(1, mo)
    r2 = 2 * nz
    for k in range(nz):
        wider[2 * k : 2 * k + 2, :] = mo[k, 0:2].astype(f32)
        wider[r2 + 2 * k : r2 + 2 * k + 2, :] = mo[k, 2:4].astype(f32)
    oslab[c, x] = wider[...].astype(bf16)
    x_spread(2, oslab)
    z_arrived(2, mz)
    for k in range(nz):
        wider[lr * k : lr * (k + 1), :] = mz[k].astype(f32)
    mslab[c, x] = wider[...].astype(bf16)
    x_spread(4, mslab)
    z_left(0, bz)
    z_left(1, mo)
    z_left(2, mz)
    bnat[...] = mul(by_latent, bslab[...].reshape(latent, 2 * rank)).astype(bf16)

    z_arrived(3, rz)
    proj = rz[0].astype(f32)
    for k in range(1, nz):
        proj = proj + rz[k].astype(f32)
    ag[z] = proj.astype(bf16)
    sz[z] = jnp.full((1, 128), jnp.sum(proj * proj), f32)
    z_spread(5, sz)
    z_spread(4, ag)

    x_onward(2, oslab)
    z_left(3, rz)
    x_left(0, bslab)
    for dx in range(1, nx):
        p = lax.rem(x + dx, nx)
        x_copy(1, xs.at[p], rx.at[x], dx).wait_send()
    for dx in range(nx):
        p = lax.rem(x + dx, nx)
        c_copy(1, dx, rounded.at[rows(other, p)], rc.at[p]).wait_send()
    x_arrived(2, oslab)
    by_rank = moved(2, (nz, nx, nc), back=True)
    for k, decay in enumerate((first_decay, second_decay)):
        old = oslab[:, :, k * r2 : (k + 1) * r2].reshape(rank, w)
        mold[k] = (decay * mul_t(old, by_rank)).reshape(nc, nx, share, rank)

    z_arrived(5, sz)
    sp[mine] = jnp.sum(sz[...], axis=0)

    def p_copy(src, dst, peer, there, here):
        return pltpu.make_async_remote_copy(
            src_ref=src, dst_ref=dst,
            send_sem=psend.at[there], recv_sem=precv.at[here],
            device_id=peer, device_id_type=MESH,
        )

    @pl.loop(1, plane)
    def _(i):
        peer, p = plane_peer(i)
        p_copy(sp.at[mine], sp.at[mine], peer, p, mine).start()

    z_arrived(4, ag)
    for k in range(nz):
        for h in range(halves):
            for j in range(pairs):
                first = 2 * (k * pairs + j)
                pt[h, first : first + 2] = ag[k, h * pairs + j].astype(f32)
    for h in range(halves):
        ps[c, x, :, h * lanes : (h + 1) * lanes] = pt[h].astype(bf16)
    x_spread(3, ps)
    z_left(4, ag)
    z_left(5, sz)
    x_left(2, oslab)

    x_onward(4, mslab)
    x_arrived(4, mslab)
    mnat[...] = mul(by_latent, mslab[...].reshape(latent, w)).astype(bf16)
    x_left(4, mslab)

    @pl.loop(1, plane)
    def _(i):
        peer, p = plane_peer(i)
        p_copy(sp.at[p], sp.at[p], peer, p, p).wait_recv()

    @pl.loop(1, plane)
    def _(i):
        peer, p = plane_peer(i)
        p_copy(sp.at[p], sp.at[p], peer, p, p).wait_send()

    mean = jnp.sum(sp[...], axis=0)[:, 0:1] / count + mean_guard
    scale = 1.0 / jnp.sqrt(mean)
    scale_out[...] = jnp.broadcast_to(scale, scale_out.shape)

    def settle(core, p):
        scaled = ps[core, p].astype(f32) * scale
        first_new = mold[0, core, p] + (1.0 - first_decay) * scaled
        second_new = mold[1, core, p] + (1.0 - second_decay) * scaled * scaled
        heads[core, p] = (first_new / (jnp.sqrt(second_new) + root_guard)).astype(bf16)

    settle(c, x)
    for dx in X_ORDER[nx][::-1]:
        p = lax.rem(x + dx, nx)
        x_from(3, ps.at[c, p], dx)
        c_copy(3, dx, ps.at[c, p], ps.at[c, p]).start()
    for dx in X_ORDER[nx][::-1]:
        settle(c, lax.rem(x + dx, nx))
    for dx in (0,) + X_ORDER[nx][::-1]:
        p = lax.rem(x + dx, nx)
        c_copy(3, dx, ps.at[other, p], ps.at[other, p]).wait_recv()
        settle(other, p)
    x_left(3, ps)


def moments(scaled, first_old, second_old):
    first = first_decay * first_old + (1.0 - first_decay) * scaled
    second = second_decay * second_old + (1.0 - second_decay) * scaled * scaled
    return first, second


def finish(sizes, *refs):
    (
        heads, proj, basis, master, scale, qb, qf, qs, kb, kf, ks,
        qf_out, qs_out, qstep_out, qcopy_out, kf_out, ks_out, kstep_out, kcopy_out,
    ) = refs
    nz, nx, nc, nt = sizes
    rank = qb.shape[1]
    qw = qf.shape[1]
    z, x, c, _ = (lax.axis_index(a) for a in AXES)
    own = 2 * ((z * nx + x) * nc + c) + lax.broadcasted_iota(jnp.int32, (8, rank), 0)
    mine = jnp.where(own == lax.broadcasted_iota(jnp.int32, (8, rank), 1), 1.0, 0.0).astype(bf16)
    scaled = mul_by_t(mine, proj[...])[:2] * scale[:, 0:1]
    qf_out[...], qs_out[...] = moments(scaled[:, :qw], qf[...], qs[...])
    kf_out[...], ks_out[...] = moments(scaled[:, qw:], kf[...], ks[...])
    q_dir = heads[:qw]
    k_dir = heads[qw:]
    qstep_out[...] = mul_by_t(qb[...], q_dir)
    kstep_out[...] = mul_by_t(kb[...], k_dir)
    q_step = mul_by_t(basis[:, :rank], q_dir)
    qcopy_out[...] = (master[:, :qw].astype(f32) - step_size * q_step).astype(bf16)
    k_step = mul_by_t(basis[:, rank:], k_dir)
    kcopy_out[...] = (master[:, qw:].astype(f32) - step_size * k_step).astype(bf16)


X_ORDER = {2: (1,), 4: (2, 1, 3)}


def body(sizes, *args):
    nz, nx, nc, nt = sizes
    args = [pltpu.with_memory_space_constraint(a, pltpu.HBM) for a in args]
    ql, qg, qm, qb, qf, qs, kl, kg, km, kb, kf, ks = args
    qw, kw = qg.shape[1], kg.shape[1]
    w = qw + kw
    fs = nz * nx * nc
    lr, rank = qb.shape
    latent = lr * fs
    count = float(rank * w * nt)
    plane = nx * nc * nt
    share = w // (nc * nx)
    lanes = min(128, rank)
    pieces = (nz, rank // lanes * (share // nz // 2), 2, lanes)
    vmem = pl.BlockSpec(memory_space=pltpu.VMEM)
    hbm = pl.BlockSpec(memory_space=pltpu.HBM)
    shape = jax.ShapeDtypeStruct
    heads, proj, basis, master, scale = pl.pallas_call(
        functools.partial(kernel, sizes, (qw, kw), count),
        out_shape=(
            shape((nc, nx, share, rank), bf16), shape((nc, nx, share, rank), bf16),
            shape((latent, 2 * rank), bf16), shape((latent, w), bf16), shape((1, 128), f32),
        ),
        in_specs=[hbm] * 12,
        out_specs=[vmem] * 5,
        scratch_shapes=[
            pltpu.VMEM(ql.shape, bf16), pltpu.VMEM(qg.shape, bf16),
            pltpu.VMEM(kl.shape, bf16), pltpu.VMEM(kg.shape, bf16),
            *(pltpu.VMEM(a.shape, f32) for a in (qm, qf, qs, km, kf, ks)),
            pltpu.VMEM((nz, lr, 2 * rank), bf16),
            pltpu.VMEM((nz, 4, w), bf16),
            pltpu.VMEM((nz, lr, w), bf16),
            pltpu.VMEM((nc, nx, nz * lr, 2 * rank), bf16),
            pltpu.VMEM((nc, nx, nz * 4, w), bf16),
            pltpu.VMEM((nc, nx, nz * lr, w), bf16),
            pltpu.VMEM((w, latent), f32),
            pltpu.VMEM((w, latent), bf16),
            pltpu.VMEM((nz * lr, 2 * rank), f32),
            pltpu.VMEM((nz * lr, w), f32),
            pltpu.VMEM((2, nc, nx, share, rank), f32),
            pltpu.VMEM((nx, share, latent), bf16),
            pltpu.VMEM((nx, share, latent), bf16),
            pltpu.VMEM((nx, share, latent), bf16),
            pltpu.VMEM((nc, 2 * share, latent // nc), bf16),
            pltpu.VMEM((rank // lanes, share, lanes), f32),
            pltpu.VMEM(pieces, bf16),
            pltpu.VMEM(pieces, bf16),
            pltpu.VMEM(pieces, bf16),
            pltpu.VMEM((plane, 1, 128), f32),
            pltpu.VMEM((nz, 1, 128), f32),
            pltpu.SemaphoreType.DMA((12,)),
            pltpu.SemaphoreType.DMA((6, nz)), pltpu.SemaphoreType.DMA((6, nz)),
            pltpu.SemaphoreType.DMA((plane,)), pltpu.SemaphoreType.DMA((plane,)),
            pltpu.SemaphoreType.DMA((5, nx)), pltpu.SemaphoreType.DMA((5, nx)),
            pltpu.SemaphoreType.DMA((5, nx)), pltpu.SemaphoreType.DMA((5, nx)),
        ],
        compiler_params=pltpu.CompilerParams(
            collective_id=0, has_side_effects=True, vmem_limit_bytes=36 * 1024 * 1024
        ),
    )(*args)
    return pl.pallas_call(
        functools.partial(finish, sizes),
        out_shape=(
            shape(qf.shape, f32), shape(qs.shape, f32), shape(qm.shape, f32), shape((latent, qw), bf16),
            shape(kf.shape, f32), shape(ks.shape, f32), shape(km.shape, f32), shape((latent, kw), bf16),
        ),
        in_specs=[vmem] * 11,
        out_specs=[vmem] * 8,
        compiler_params=pltpu.CompilerParams(vmem_limit_bytes=20 * 1024 * 1024),
    )(heads.reshape(w, rank), proj.reshape(w, rank), basis, master, scale, qb, qf, qs, kb, kf, ks)


def solution(mesh, chips=(16, 4, 2)):
    nt = mesh.shape["tp"]
    finer = Mesh(mesh.devices.reshape(*chips, nt), AXES)
    in_specs = (P(FS, None), P(FS, "t"), P(FS, "t"), P(FS, None), P(FS, "t"), P(FS, "t")) * 2
    out_specs = (P(FS, "t"), P(FS, "t"), P(FS, "t"), P(None, "t")) * 2
    return jax.shard_map(
        functools.partial(body, (*chips, nt)), mesh=finer, in_specs=in_specs, out_specs=out_specs, check_vma=False
    )
```

```python
import functools

import jax
import jax.numpy as jnp
from jax import lax
from jax.experimental import pallas as pl
from jax.experimental.pallas import tpu as pltpu
from jax.sharding import Mesh
from jax.sharding import PartitionSpec as P

AXES = ("z", "x", "c", "t")
FS = ("z", "x", "c")
MESH = pl.DeviceIdType.MESH
f32 = jnp.float32
bf16 = jnp.bfloat16

first_decay = 0.8
second_decay = 0.9
step_size = 0.5
mean_guard = 1e-06
root_guard = 1e-08


def log2(n):
    return n.bit_length() - 1


def part(v, low, size):
    return lax.shift_right_logical(v, low) & (size - 1)


def moved(rows, sizes, back=False):
    nz, nx, nc = sizes
    n = nz * nx * nc * rows
    lr, lz, lx, lc = log2(rows), log2(nz), log2(nx), log2(nc)
    nat = lax.broadcasted_iota(jnp.int32, (n, n), int(back))
    got = lax.broadcasted_iota(jnp.int32, (n, n), 1 - int(back))
    r = part(got, 0, rows)
    z = part(got, lr, nz)
    x = part(got, lr + lz, nx)
    c = part(got, lr + lz + lx, nc)
    want = ((z * nx + x) * nc + c) * rows + r
    return jnp.where(nat == want, 1.0, 0.0).astype(bf16)


def mul(a, b):
    return jnp.dot(a, b, preferred_element_type=f32)


def mul_by_t(a, b):
    return lax.dot_general(a, b, (((1,), (1,)), ((), ())), preferred_element_type=f32)


def mul_t(a, b):
    return lax.dot_general(a, b, (((0,), (0,)), ((), ())), preferred_element_type=f32)


def kernel(sizes, widths, count, *refs):
    nz, nx, nc, nt = sizes
    qw, kw = widths
    (
        ql, qg, qm_h, qb, qf_h, qs_h, kl, kg, km_h, kb, kf_h, ks_h,
        heads, ps, bnat, mnat, scale_out, qb_v, qf, qs, kb_v, kf, ks,
        ql_v, qg_v, kl_v, kg_v, qm, km,
        bz, mm, bslab, oslab, mslab, tokens, rounded, wide, wider, mold,
        rc, xs, rx, hilo, pt, zs, rz, ag, sp, sz,
        load_sem, zsend, zrecv, psend, precv, xsend, xrecv, csend, crecv,
    ) = refs
    w = qw + kw
    rank = qb.shape[1]
    lr = bz.shape[1]
    latent = lr * nz * nx * nc
    share = w // (nc * nx)
    lanes = pt.shape[2]
    halves = rank // lanes
    pairs = share // nz // 2
    z, x, c, t = (lax.axis_index(a) for a in AXES)
    other = 1 - c

    loads = [
        pltpu.make_async_copy(src, dst, load_sem.at[k])
        for k, (src, dst) in enumerate((
            (ql, ql_v), (qg, qg_v), (kl, kl_v), (kg, kg_v),
            (qb, bz.at[z, :, :rank]), (kb, bz.at[z, :, rank:]),
            (qf_h, qf), (qs_h, qs), (kf_h, kf), (ks_h, ks), (qm_h, qm), (km_h, km),
            (qb, qb_v), (kb, kb_v),
        ))
    ]

    barrier = pltpu.get_barrier_semaphore()
    plane = nx * nc * nt
    mine = (x * nc + c) * nt + t

    along = [nz // 2] + [nz // 2 + h * side for h in range(1, nz // 2) for side in (1, -1)]
    peers = [lax.rem(z + d, nz) for d in along]
    xp = [lax.rem(x + d, nx) for d in range(nx)]
    tp = [lax.rem(t + d, nt) for d in range(nt)]
    around = [
        (z, xp[dx], core, tp[dt])
        for dx in range(nx) for dt in range(nt) for core in (c, other)
        if dx or dt or core is other
    ]

    for p in peers:
        pl.semaphore_signal(barrier, inc=1, device_id=(p, x, c, t), device_id_type=MESH)
    for load in loads:
        load.start()
    for peer in around:
        pl.semaphore_signal(barrier, inc=1, device_id=peer, device_id_type=MESH)

    def z_copy(stage, src, dst, peer):
        return pltpu.make_async_remote_copy(
            src_ref=src, dst_ref=dst, send_sem=zsend.at[stage], recv_sem=zrecv.at[stage],
            device_id=(peer, x, c, t), device_id_type=MESH,
        )

    def z_spread(stage, buf):
        for p in peers:
            z_copy(stage, buf.at[z], buf.at[z], p).start()

    def z_all(stage, buf, n=nz - 1):
        return z_copy(stage, buf.at[pl.ds(0, n)], buf.at[pl.ds(0, n)], peers[0])

    def x_copy(stage, src, dst, dx):
        p = lax.rem(x + dx, nx)
        return pltpu.make_async_remote_copy(
            src_ref=src, dst_ref=dst,
            send_sem=xsend.at[stage, dx], recv_sem=xrecv.at[stage, nx - dx],
            device_id=(z, p, c, t), device_id_type=MESH,
        )

    def x_from(stage, buf, dx):
        pltpu.make_async_remote_copy(
            src_ref=buf, dst_ref=buf,
            send_sem=xsend.at[stage, dx], recv_sem=xrecv.at[stage, dx],
            device_id=(z, lax.rem(x + dx, nx), c, t), device_id_type=MESH,
        ).wait_recv()

    def c_copy(stage, k, src, dst):
        return pltpu.make_async_remote_copy(
            src_ref=src, dst_ref=dst,
            send_sem=csend.at[stage, k], recv_sem=crecv.at[stage, k],
            device_id=(z, x, other, t), device_id_type=MESH,
        )

    def x_spread(stage, slabs):
        for dx in X_ORDER[nx]:
            x_copy(stage, slabs.at[c, x], slabs.at[c, x], dx).start()
        c_copy(stage, 0, slabs.at[c, x], slabs.at[c, x]).start()

    def x_onward(stage, slabs):
        for dx in X_ORDER[nx][::-1]:
            p = lax.rem(x + dx, nx)
            x_from(stage, slabs.at[c, p], dx)
            c_copy(stage, dx, slabs.at[c, p], slabs.at[c, p]).start()

    def x_arrived(stage, slabs):
        for dx in range(nx):
            p = lax.rem(x + dx, nx)
            c_copy(stage, dx, slabs.at[other, p], slabs.at[other, p]).wait_recv()

    def x_left(stage, slabs):
        for dx in range(1, nx):
            x_copy(stage, slabs.at[c, x], slabs.at[c, x], dx).wait_send()
        for dx in range(nx):
            p = lax.rem(x + dx, nx)
            c_copy(stage, dx, slabs.at[c, p], slabs.at[c, p]).wait_send()

    def rows(core, p):
        return pl.ds(pl.multiple_of((core * nx + p) * share, share), share)

    for load in loads[:2]:
        load.wait()
    tokens[:qw] = mul_t(qg_v[...], ql_v[...])
    for load in loads[2:4]:
        load.wait()
    tokens[qw:] = mul_t(kg_v[...], kl_v[...])
    rounded[...] = tokens[...].astype(bf16)
    for load in loads[4:]:
        load.wait()
    zr, zq = lax.rem(z, 4), z // 4
    mm[zr, zq, 0:2, :qw] = qf[...].astype(bf16)
    mm[zr, zq, 0:2, qw:] = kf[...].astype(bf16)
    mm[zr, zq, 2:4, :qw] = qs[...].astype(bf16)
    mm[zr, zq, 2:4, qw:] = ks[...].astype(bf16)
    mm[zr, zq, 4:8, :qw] = qm[...].astype(bf16)
    mm[zr, zq, 4:8, qw:] = km[...].astype(bf16)
    pl.semaphore_wait(barrier, nz - 1 + plane - 1)

    order = X_ORDER[nx] + (0,)
    z_spread(0, bz)
    for dx in order:
        p = lax.rem(x + dx, nx)
        c_copy(1, dx, rounded.at[rows(other, p)], rc.at[p]).start()
    for dx in order:
        p = lax.rem(x + dx, nx)
        c_copy(1, dx, rc.at[p], rc.at[p]).wait_recv()
        both = tokens[rows(c, p)] + rc[p].astype(f32)
        if dx:
            xs[p] = both.astype(bf16)
            x_copy(1, xs.at[p], rx.at[x], dx).start()
        else:
            tokens[rows(c, p)] = both

    for k in range(1, nz // 4):
        z_copy(1, mm.at[zr, zq], mm.at[zr, zq], lax.rem(z + 4 * k, nz)).start()
    by_latent = moved(lr, (nz, nx, nc))

    z_all(0, bz).wait_recv()
    for k in range(nz):
        wide[lr * k : lr * (k + 1), :] = bz[k].astype(f32)
    bslab[c, x] = wide[...].astype(bf16)
    x_spread(0, bslab)
    if nz > 4:
        z_all(1, mm.at[0], nz // 4 - 1).wait_recv()
    for d in (2, 1, nz - 1):
        z_copy(2, mm.at[zr], mm.at[zr], lax.rem(z + d, nz)).start()

    total = tokens[rows(c, x)]
    for dx in range(1, nx):
        p = lax.rem(x + dx, nx)
        x_from(1, rx.at[p], dx)
        total = total + rx[p].astype(f32)
    high = total.astype(bf16)
    low = (total - high.astype(f32)).astype(bf16)
    part_of = latent // nc
    turned_high = mul(high, by_latent).astype(bf16)
    turned_low = mul(low, by_latent).astype(bf16)
    for k in range(nc):
        hilo[k, :share] = turned_high[:, k * part_of : (k + 1) * part_of]
        hilo[k, share:] = turned_low[:, k * part_of : (k + 1) * part_of]

    x_onward(0, bslab)
    got = mul(hilo[c], bslab[c].reshape(part_of, 2 * rank))
    x_arrived(0, bslab)
    got = got + mul(hilo[other], bslab[other].reshape(part_of, 2 * rank))
    got = got[:share] + got[share:]
    column = (c * nx + x) * share + lax.broadcasted_iota(jnp.int32, (share, rank), 0)
    got = jnp.where(column < qw, got[:, :rank], got[:, rank:])
    for h in range(halves):
        pt[h] = got[:, h * lanes : (h + 1) * lanes]
    for k in range(nz):
        for h in range(halves):
            for j in range(pairs):
                first = 2 * (k * pairs + j)
                zs[k, h * pairs + j] = pt[h, first : first + 2].astype(bf16)

    for p in peers:
        z_copy(3, zs.at[p], rz.at[z], p).start()
    rz[z] = zs[z]

    z_all(2, mm, 3).wait_recv()
    r2 = 2 * nz
    for k in range(nz):
        wider[2 * k : 2 * k + 2, :] = mm[k % 4, k // 4, 0:2].astype(f32)
        wider[r2 + 2 * k : r2 + 2 * k + 2, :] = mm[k % 4, k // 4, 2:4].astype(f32)
    oslab[c, x] = wider[...].astype(bf16)
    x_spread(2, oslab)
    for k in range(nz):
        wider[lr * k : lr * (k + 1), :] = mm[k % 4, k // 4, 4:8].astype(f32)
    mslab[c, x] = wider[...].astype(bf16)
    x_spread(4, mslab)
    z_all(0, bz).wait_send()
    if nz > 4:
        z_all(1, mm.at[0], nz // 4 - 1).wait_send()
    z_all(2, mm, 3).wait_send()
    bnat[...] = mul(by_latent, bslab[...].reshape(latent, 2 * rank)).astype(bf16)

    z_all(3, rz).wait_recv()
    proj = rz[0].astype(f32)
    for k in range(1, nz):
        proj = proj + rz[k].astype(f32)
    ag[z] = proj.astype(bf16)
    sz[z] = jnp.full((1, 128), jnp.sum(proj * proj), f32)
    z_spread(4, ag)
    z_spread(5, sz)

    x_onward(2, oslab)
    z_all(3, zs).wait_send()
    x_left(0, bslab)
    for dx in range(1, nx):
        p = lax.rem(x + dx, nx)
        x_copy(1, xs.at[p], rx.at[x], dx).wait_send()
    for dx in range(nx):
        p = lax.rem(x + dx, nx)
        c_copy(1, dx, rounded.at[rows(other, p)], rc.at[p]).wait_send()
    x_arrived(2, oslab)
    by_rank = moved(2, (nz, nx, nc), back=True)
    for k, decay in enumerate((first_decay, second_decay)):
        old = oslab[:, :, k * r2 : (k + 1) * r2].reshape(rank, w)
        mold[k] = (decay * mul_t(old, by_rank)).reshape(nc, nx, share, rank)

    z_all(5, sz).wait_recv()
    sp[mine] = jnp.sum(sz[...], axis=0)

    def p_copy(src, dst, peer):
        return pltpu.make_async_remote_copy(
            src_ref=src, dst_ref=dst, send_sem=psend.at[0], recv_sem=precv.at[0],
            device_id=peer, device_id_type=MESH,
        )

    for peer in around:
        p_copy(sp.at[mine], sp.at[mine], peer).start()

    z_all(4, ag).wait_recv()
    for k in range(nz):
        for h in range(halves):
            for j in range(pairs):
                first = 2 * (k * pairs + j)
                pt[h, first : first + 2] = ag[k, h * pairs + j].astype(f32)
    for h in range(halves):
        ps[c, x, :, h * lanes : (h + 1) * lanes] = pt[h].astype(bf16)
    x_spread(3, ps)
    z_all(4, ag).wait_send()
    z_all(5, sz).wait_send()
    x_left(2, oslab)

    x_onward(4, mslab)
    x_arrived(4, mslab)
    mnat[...] = mul(by_latent, mslab[...].reshape(latent, w)).astype(bf16)
    x_left(4, mslab)

    everyone = sp.at[pl.ds(0, plane - 1)]
    p_copy(everyone, everyone, around[0]).wait_recv()
    p_copy(everyone, everyone, around[0]).wait_send()

    mean = jnp.sum(sp[...], axis=0)[:, 0:1] / count + mean_guard
    scale = 1.0 / jnp.sqrt(mean)
    scale_out[...] = jnp.broadcast_to(scale, scale_out.shape)

    def settle(core, p):
        scaled = ps[core, p].astype(f32) * scale
        first_new = mold[0, core, p] + (1.0 - first_decay) * scaled
        second_new = mold[1, core, p] + (1.0 - second_decay) * scaled * scaled
        heads[core, p] = (first_new / (jnp.sqrt(second_new) + root_guard)).astype(bf16)

    settle(c, x)
    for dx in X_ORDER[nx][::-1]:
        p = lax.rem(x + dx, nx)
        x_from(3, ps.at[c, p], dx)
        c_copy(3, dx, ps.at[c, p], ps.at[c, p]).start()
    for dx in X_ORDER[nx][::-1]:
        settle(c, lax.rem(x + dx, nx))
    for dx in (0,) + X_ORDER[nx][::-1]:
        p = lax.rem(x + dx, nx)
        c_copy(3, dx, ps.at[other, p], ps.at[other, p]).wait_recv()
        settle(other, p)
    x_left(3, ps)


def moments(scaled, first_old, second_old):
    first = first_decay * first_old + (1.0 - first_decay) * scaled
    second = second_decay * second_old + (1.0 - second_decay) * scaled * scaled
    return first, second


def finish(sizes, *refs):
    (
        heads, proj, basis, master, scale, qb, qf, qs, kb, kf, ks,
        qf_out, qs_out, qstep_out, qcopy_out, kf_out, ks_out, kstep_out, kcopy_out,
        fresh_q, fresh_k, sems,
    ) = refs
    nz, nx, nc, nt = sizes
    rank = qb.shape[1]
    qw = qf.shape[1]
    z, x, c, _ = (lax.axis_index(a) for a in AXES)
    q_dir = heads[:qw]
    k_dir = heads[qw:]
    latent = basis.shape[0]
    cut = latent // 2
    copies = []
    for columns, towards, old, fresh, out in (
        (slice(0, rank), q_dir, slice(0, qw), fresh_q, qcopy_out),
        (slice(rank, 2 * rank), k_dir, slice(qw, master.shape[1]), fresh_k, kcopy_out),
    ):
        for k in range(2):
            some = slice(k * cut, (k + 1) * cut)
            step = mul_by_t(basis[some, columns], towards)
            fresh[some] = (master[some, old].astype(f32) - step_size * step).astype(bf16)
            copies.append(pltpu.make_async_copy(fresh.at[some], out.at[some], sems.at[len(copies)]))
            copies[-1].start()
    own = 2 * ((z * nx + x) * nc + c) + lax.broadcasted_iota(jnp.int32, (8, rank), 0)
    mine = jnp.where(own == lax.broadcasted_iota(jnp.int32, (8, rank), 1), 1.0, 0.0).astype(bf16)
    scaled = mul_by_t(mine, proj[...])[:2] * scale[:, 0:1]
    qf_out[...], qs_out[...] = moments(scaled[:, :qw], qf[...], qs[...])
    kf_out[...], ks_out[...] = moments(scaled[:, qw:], kf[...], ks[...])
    qstep_out[...] = mul_by_t(qb[...], q_dir)
    kstep_out[...] = mul_by_t(kb[...], k_dir)
    for copy in copies:
        copy.wait()


X_ORDER = {2: (1,), 4: (2, 1, 3)}


def body(sizes, *args):
    nz, nx, nc, nt = sizes
    args = [pltpu.with_memory_space_constraint(a, pltpu.HBM) for a in args]
    ql, qg, qm, qb, qf, qs, kl, kg, km, kb, kf, ks = args
    qw, kw = qg.shape[1], kg.shape[1]
    w = qw + kw
    fs = nz * nx * nc
    lr, rank = qb.shape
    latent = lr * fs
    count = float(rank * w * nt)
    plane = nx * nc * nt
    share = w // (nc * nx)
    lanes = min(128, rank)
    pieces = (nz, rank // lanes * (share // nz // 2), 2, lanes)
    vmem = pl.BlockSpec(memory_space=pltpu.VMEM)
    hbm = pl.BlockSpec(memory_space=pltpu.HBM)
    shape = jax.ShapeDtypeStruct
    heads, proj, basis, master, scale, *small = pl.pallas_call(
        functools.partial(kernel, sizes, (qw, kw), count),
        out_shape=(
            shape((nc, nx, share, rank), bf16), shape((nc, nx, share, rank), bf16),
            shape((latent, 2 * rank), bf16), shape((latent, w), bf16), shape((1, 128), f32),
            *(shape(a.shape, a.dtype) for a in (qb, qf, qs, kb, kf, ks)),
        ),
        in_specs=[hbm] * 12,
        out_specs=[vmem] * 11,
        scratch_shapes=[
            pltpu.VMEM(ql.shape, bf16), pltpu.VMEM(qg.shape, bf16),
            pltpu.VMEM(kl.shape, bf16), pltpu.VMEM(kg.shape, bf16),
            *(pltpu.VMEM(a.shape, f32) for a in (qm, km)),
            pltpu.VMEM((nz, lr, 2 * rank), bf16),
            pltpu.VMEM((4, nz // 4, 8, w), bf16),
            pltpu.VMEM((nc, nx, nz * lr, 2 * rank), bf16),
            pltpu.VMEM((nc, nx, nz * 4, w), bf16),
            pltpu.VMEM((nc, nx, nz * lr, w), bf16),
            pltpu.VMEM((w, latent), f32),
            pltpu.VMEM((w, latent), bf16),
            pltpu.VMEM((nz * lr, 2 * rank), f32),
            pltpu.VMEM((nz * lr, w), f32),
            pltpu.VMEM((2, nc, nx, share, rank), f32),
            pltpu.VMEM((nx, share, latent), bf16),
            pltpu.VMEM((nx, share, latent), bf16),
            pltpu.VMEM((nx, share, latent), bf16),
            pltpu.VMEM((nc, 2 * share, latent // nc), bf16),
            pltpu.VMEM((rank // lanes, share, lanes), f32),
            pltpu.VMEM(pieces, bf16),
            pltpu.VMEM(pieces, bf16),
            pltpu.VMEM(pieces, bf16),
            pltpu.VMEM((plane, 1, 128), f32),
            pltpu.VMEM((nz, 1, 128), f32),
            pltpu.SemaphoreType.DMA((14,)),
            pltpu.SemaphoreType.DMA((6,)), pltpu.SemaphoreType.DMA((6,)),
            pltpu.SemaphoreType.DMA((1,)), pltpu.SemaphoreType.DMA((1,)),
            pltpu.SemaphoreType.DMA((5, nx)), pltpu.SemaphoreType.DMA((5, nx)),
            pltpu.SemaphoreType.DMA((5, nx)), pltpu.SemaphoreType.DMA((5, nx)),
        ],
        compiler_params=pltpu.CompilerParams(
            collective_id=0, has_side_effects=True, vmem_limit_bytes=36 * 1024 * 1024
        ),
    )(*args)
    return pl.pallas_call(
        functools.partial(finish, sizes),
        out_shape=(
            shape(qf.shape, f32), shape(qs.shape, f32), shape(qm.shape, f32), shape((latent, qw), bf16),
            shape(kf.shape, f32), shape(ks.shape, f32), shape(km.shape, f32), shape((latent, kw), bf16),
        ),
        in_specs=[vmem] * 11,
        out_specs=[vmem, vmem, vmem, hbm] * 2,
        scratch_shapes=[
            pltpu.VMEM((latent, qw), bf16), pltpu.VMEM((latent, kw), bf16), pltpu.SemaphoreType.DMA((4,)),
        ],
        compiler_params=pltpu.CompilerParams(vmem_limit_bytes=20 * 1024 * 1024),
    )(heads.reshape(w, rank), proj.reshape(w, rank), basis, master, scale, *small)


def solution(mesh, chips=(16, 4, 2)):
    nt = mesh.shape["tp"]
    finer = Mesh(mesh.devices.reshape(*chips, nt), AXES)
    in_specs = (P(FS, None), P(FS, "t"), P(FS, "t"), P(FS, None), P(FS, "t"), P(FS, "t")) * 2
    out_specs = (P(FS, "t"), P(FS, "t"), P(FS, "t"), P(None, "t")) * 2
    return jax.shard_map(
        functools.partial(body, (*chips, nt)), mesh=finer, in_specs=in_specs, out_specs=out_specs, check_vma=False
    )
```

```python
import functools

import jax
import jax.numpy as jnp
from jax import lax
from jax.experimental import pallas as pl
from jax.experimental.pallas import tpu as pltpu
from jax.sharding import Mesh
from jax.sharding import PartitionSpec as P

AXES = ("z", "x", "c", "t")
FS = ("z", "x", "c")
MESH = pl.DeviceIdType.MESH
f32 = jnp.float32
bf16 = jnp.bfloat16

first_decay = 0.8
second_decay = 0.9
step_size = 0.5
mean_guard = 1e-06
root_guard = 1e-08


def log2(n):
    return n.bit_length() - 1


def part(v, low, size):
    return lax.shift_right_logical(v, low) & (size - 1)


def moved(rows, sizes, back=False):
    nz, nx, nc = sizes
    n = nz * nx * nc * rows
    lr, lz, lx, lc = log2(rows), log2(nz), log2(nx), log2(nc)
    nat = lax.broadcasted_iota(jnp.int32, (n, n), int(back))
    got = lax.broadcasted_iota(jnp.int32, (n, n), 1 - int(back))
    r = part(got, 0, rows)
    z = part(got, lr, nz)
    x = part(got, lr + lz, nx)
    c = part(got, lr + lz + lx, nc)
    want = ((z * nx + x) * nc + c) * rows + r
    return jnp.where(nat == want, 1.0, 0.0).astype(bf16)


def mul(a, b):
    return jnp.dot(a, b, preferred_element_type=f32)


def mul_by_t(a, b):
    return lax.dot_general(a, b, (((1,), (1,)), ((), ())), preferred_element_type=f32)


def mul_t(a, b):
    return lax.dot_general(a, b, (((0,), (0,)), ((), ())), preferred_element_type=f32)


def kernel(sizes, widths, count, *refs):
    nz, nx, nc, nt = sizes
    qw, kw = widths
    (
        ql, qg, qm_h, qb, qf_h, qs_h, kl, kg, km_h, kb, kf_h, ks_h,
        heads, ps, bnat, mnat, scale_out, qb_v, qf, qs, kb_v, kf, ks,
        ql_v, qg_v, kl_v, kg_v, qm, km,
        bz, mm, bslab, oslab, mslab, tokens, rounded, wide, wider, mold,
        rc, xs, rx, relay, hilo, pt, zs, rz, ag, sp, sz,
        load_sem, zsend, zrecv, psend, precv, xsend, xrecv, csend, crecv, rsend, rrecv, bsend, brecv,
    ) = refs
    w = qw + kw
    rank = qb.shape[1]
    lr = bz.shape[1]
    latent = lr * nz * nx * nc
    share = w // (nc * nx)
    lanes = pt.shape[2]
    halves = rank // lanes
    pairs = share // nz // 2
    z, x, c, t = (lax.axis_index(a) for a in AXES)
    other = 1 - c

    loads = [
        pltpu.make_async_copy(src, dst, load_sem.at[k])
        for k, (src, dst) in enumerate((
            (ql, ql_v), (qg, qg_v), (kl, kl_v), (kg, kg_v),
            (qb, bz.at[z, :, :rank]), (kb, bz.at[z, :, rank:]),
            (qf_h, qf), (qs_h, qs), (kf_h, kf), (ks_h, ks), (qm_h, qm), (km_h, km),
            (qb, qb_v), (kb, kb_v),
        ))
    ]

    barrier = pltpu.get_barrier_semaphore()
    plane = nx * nc * nt
    mine = (x * nc + c) * nt + t

    along = [nz // 2] + [nz // 2 + h * side for h in range(1, nz // 2) for side in (1, -1)]
    peers = [lax.rem(z + d, nz) for d in along]
    xp = [lax.rem(x + d, nx) for d in range(nx)]
    tp = [lax.rem(t + d, nt) for d in range(nt)]
    around = [
        (z, xp[dx], core, tp[dt])
        for dx in range(nx) for dt in range(nt) for core in (c, other)
        if dx or dt or core is other
    ]

    for p in peers:
        pl.semaphore_signal(barrier, inc=1, device_id=(p, x, c, t), device_id_type=MESH)
    for load in loads:
        load.start()
    for peer in around:
        pl.semaphore_signal(barrier, inc=1, device_id=peer, device_id_type=MESH)

    def z_copy(stage, src, dst, peer):
        return pltpu.make_async_remote_copy(
            src_ref=src, dst_ref=dst, send_sem=zsend.at[stage], recv_sem=zrecv.at[stage],
            device_id=(peer, x, c, t), device_id_type=MESH,
        )

    def z_spread(stage, buf):
        for p in peers:
            z_copy(stage, buf.at[z], buf.at[z], p).start()

    def z_all(stage, buf, n=nz - 1):
        return z_copy(stage, buf.at[pl.ds(0, n)], buf.at[pl.ds(0, n)], peers[0])

    def x_copy(stage, src, dst, dx):
        p = lax.rem(x + dx, nx)
        return pltpu.make_async_remote_copy(
            src_ref=src, dst_ref=dst,
            send_sem=xsend.at[stage // 3, dx], recv_sem=xrecv.at[stage // 3, nx - dx],
            device_id=(z, p, c, t), device_id_type=MESH,
        )

    def x_from(stage, buf, dx):
        pltpu.make_async_remote_copy(
            src_ref=buf, dst_ref=buf,
            send_sem=xsend.at[stage // 3, dx], recv_sem=xrecv.at[stage // 3, dx],
            device_id=(z, lax.rem(x + dx, nx), c, t), device_id_type=MESH,
        ).wait_recv()

    right, across, left = xp[1], xp[2], xp[3]
    half = share // 2
    ahead, behind = pl.ds(0, half), pl.ds(half, half)

    def beside(sends, recvs, k, rightward, src, dst):
        return pltpu.make_async_remote_copy(
            src_ref=src, dst_ref=dst, send_sem=sends.at[k], recv_sem=recvs.at[k],
            device_id=(z, right if rightward else left, c, t), device_id_type=MESH,
        )

    def c_copy(stage, k, src, dst):
        return pltpu.make_async_remote_copy(
            src_ref=src, dst_ref=dst,
            send_sem=csend.at[stage, k], recv_sem=crecv.at[stage, k],
            device_id=(z, x, other, t), device_id_type=MESH,
        )

    def x_spread(stage, slabs):
        for dx in X_ORDER[nx]:
            x_copy(stage, slabs.at[c, x], slabs.at[c, x], dx).start()
        c_copy(stage, 0, slabs.at[c, x], slabs.at[c, x]).start()

    def x_onward(stage, slabs):
        for dx in X_ORDER[nx][::-1]:
            p = lax.rem(x + dx, nx)
            x_from(stage, slabs.at[c, p], dx)
            c_copy(stage, dx, slabs.at[c, p], slabs.at[c, p]).start()

    def x_arrived(stage, slabs):
        for dx in range(nx):
            p = lax.rem(x + dx, nx)
            c_copy(stage, dx, slabs.at[other, p], slabs.at[other, p]).wait_recv()

    def x_left(stage, slabs):
        for dx in range(1, nx):
            x_copy(stage, slabs.at[c, x], slabs.at[c, x], dx).wait_send()
        for dx in range(nx):
            p = lax.rem(x + dx, nx)
            c_copy(stage, dx, slabs.at[c, p], slabs.at[c, p]).wait_send()

    def rows(core, p):
        return pl.ds(pl.multiple_of((core * nx + p) * share, share), share)

    for load in loads[:2]:
        load.wait()
    tokens[:qw] = mul_t(qg_v[...], ql_v[...])
    for load in loads[2:4]:
        load.wait()
    tokens[qw:] = mul_t(kg_v[...], kl_v[...])
    rounded[...] = tokens[...].astype(bf16)
    for load in loads[4:]:
        load.wait()
    zr, zq = lax.rem(z, 4), z // 4
    mm[zr, zq, 0:2, :qw] = qf[...].astype(bf16)
    mm[zr, zq, 0:2, qw:] = kf[...].astype(bf16)
    mm[zr, zq, 2:4, :qw] = qs[...].astype(bf16)
    mm[zr, zq, 2:4, qw:] = ks[...].astype(bf16)
    mm[zr, zq, 4:8, :qw] = qm[...].astype(bf16)
    mm[zr, zq, 4:8, qw:] = km[...].astype(bf16)
    pl.semaphore_wait(barrier, nz - 1 + plane - 1)

    order = X_ORDER[nx] + (0,)
    z_spread(0, bz)
    for dx in order:
        p = lax.rem(x + dx, nx)
        c_copy(1, dx, rounded.at[rows(other, p)], rc.at[p]).start()

    sums = (
        beside(rsend, rrecv, 0, True, xs.at[across, ahead], relay.at[0]),
        beside(rsend, rrecv, 1, False, xs.at[across, behind], relay.at[1]),
        beside(rsend, rrecv, 2, True, xs.at[right, behind], rx.at[0, behind]),
        beside(rsend, rrecv, 3, False, xs.at[left, ahead], rx.at[1, ahead]),
        beside(rsend, rrecv, 4, True, xs.at[right, ahead], rx.at[0, ahead]),
        beside(rsend, rrecv, 5, False, xs.at[left, behind], rx.at[1, behind]),
    )
    for dx in order:
        p = xp[dx]
        c_copy(1, dx, rc.at[p], rc.at[p]).wait_recv()
        both = tokens[rows(c, p)] + rc[p].astype(f32)
        if dx == 2:
            xs[p] = both.astype(bf16)
            sums[0].start()
            sums[1].start()
        elif dx == 1:
            xs[p, half:] = both[half:].astype(bf16)
            sums[2].start()
            tokens[rows(c, p)] = both
        elif dx == 3:
            xs[p, :half] = both[:half].astype(bf16)
            sums[3].start()
            tokens[rows(c, p)] = both
        else:
            tokens[rows(c, p)] = both

    for k in range(1, nz // 4):
        z_copy(1, mm.at[zr, zq], mm.at[zr, zq], lax.rem(z + 4 * k, nz)).start()
    by_latent = moved(lr, (nz, nx, nc))

    sums[0].wait_recv()
    passed = tokens[rows(c, right)]
    xs[right, :half] = (passed[:half] + relay[0].astype(f32)).astype(bf16)
    sums[4].start()
    sums[1].wait_recv()
    passed = tokens[rows(c, left)]
    xs[left, half:] = (passed[half:] + relay[1].astype(f32)).astype(bf16)
    sums[5].start()

    z_all(0, bz).wait_recv()
    for k in range(nz):
        wide[lr * k : lr * (k + 1), :] = bz[k].astype(f32)
    bslab[c, x] = wide[...].astype(bf16)
    x_spread(0, bslab)

    total = tokens[rows(c, x)]
    for k in range(2, 6):
        sums[k].wait_recv()
    total = total + rx[0].astype(f32) + rx[1].astype(f32)
    high = total.astype(bf16)
    low = (total - high.astype(f32)).astype(bf16)
    part_of = latent // nc
    turned_high = mul(high, by_latent).astype(bf16)
    turned_low = mul(low, by_latent).astype(bf16)
    for k in range(nc):
        hilo[k, :share] = turned_high[:, k * part_of : (k + 1) * part_of]
        hilo[k, share:] = turned_low[:, k * part_of : (k + 1) * part_of]

    fours = nz // 4
    if fours > 1:
        z_all(1, mm.at[0], fours - 1).wait_recv()
    for d, some in (
        (2, pl.ds(0, (fours + 1) // 2)), (nz - 2, pl.ds((fours + 1) // 2, fours // 2)),
        (1, pl.ds(0, fours)), (nz - 1, pl.ds(0, fours)),
    ):
        if some.size:
            z_copy(2, mm.at[zr, some], mm.at[zr, some], lax.rem(z + d, nz)).start()

    x_onward(0, bslab)
    got = mul(hilo[c], bslab[c].reshape(part_of, 2 * rank))
    x_arrived(0, bslab)
    got = got + mul(hilo[other], bslab[other].reshape(part_of, 2 * rank))
    got = got[:share] + got[share:]
    column = (c * nx + x) * share + lax.broadcasted_iota(jnp.int32, (share, rank), 0)
    got = jnp.where(column < qw, got[:, :rank], got[:, rank:])
    for h in range(halves):
        pt[h] = got[:, h * lanes : (h + 1) * lanes]
    for k in range(nz):
        for h in range(halves):
            for j in range(pairs):
                first = 2 * (k * pairs + j)
                zs[k, h * pairs + j] = pt[h, first : first + 2].astype(bf16)

    for p in peers:
        z_copy(3, zs.at[p], rz.at[z], p).start()
    rz[z] = zs[z]

    z_all(2, mm, 3).wait_recv()
    r2 = 2 * nz
    for k in range(nz):
        wider[2 * k : 2 * k + 2, :] = mm[k % 4, k // 4, 0:2].astype(f32)
        wider[r2 + 2 * k : r2 + 2 * k + 2, :] = mm[k % 4, k // 4, 2:4].astype(f32)
    oslab[c, x] = wider[...].astype(bf16)
    for k in range(nz):
        wider[lr * k : lr * (k + 1), :] = mm[k % 4, k // 4, 4:8].astype(f32)
    mslab[c, x] = wider[...].astype(bf16)
    bulk = (
        beside(bsend, brecv, 0, True, oslab.at[c, x], oslab.at[c, x]),
        beside(bsend, brecv, 1, False, mslab.at[c, x], mslab.at[c, x]),
        beside(bsend, brecv, 2, True, mslab.at[c, x], mslab.at[c, x]),
        beside(bsend, brecv, 3, False, oslab.at[c, x], oslab.at[c, x]),
        beside(bsend, brecv, 4, True, oslab.at[c, left], oslab.at[c, left]),
        beside(bsend, brecv, 5, False, mslab.at[c, right], mslab.at[c, right]),
    )
    landing = (
        (0, True, oslab, left, 3), (1, False, mslab, right, 1), (2, True, mslab, left, 3),
        (3, False, oslab, right, 1), (4, True, oslab, across, 2), (5, False, mslab, across, 2),
    )

    def c_bulk(slabs, dx, p):
        return c_copy(2 if slabs is oslab else 4, dx, slabs.at[c, p], slabs.at[c, p])

    def bulk_onward(which):
        for k in which:
            _, rightward, slabs, p, dx = landing[k]
            beside(bsend, brecv, k, rightward, slabs.at[c, p], slabs.at[c, p]).wait_recv()
            if k < 2:
                bulk[4 + k].start()
            c_bulk(slabs, dx, p).start()

    for copy in bulk[:4]:
        copy.start()
    c_bulk(oslab, 0, x).start()
    c_bulk(mslab, 0, x).start()
    z_all(0, bz).wait_send()
    if nz > 4:
        z_all(1, mm.at[0], nz // 4 - 1).wait_send()
    z_all(2, mm, 3).wait_send()
    bnat[...] = mul(by_latent, bslab[...].reshape(latent, 2 * rank)).astype(bf16)

    z_all(3, rz).wait_recv()
    proj = rz[0].astype(f32)
    for k in range(1, nz):
        proj = proj + rz[k].astype(f32)
    ag[z] = proj.astype(bf16)
    sz[z] = jnp.full((1, 128), jnp.sum(proj * proj), f32)
    z_spread(4, ag)
    z_spread(5, sz)

    bulk_onward((0, 1, 2, 3))
    z_all(3, zs).wait_send()
    x_left(0, bslab)
    for copy in sums:
        copy.wait_send()
    for dx in range(nx):
        p = xp[dx]
        c_copy(1, dx, rounded.at[rows(other, p)], rc.at[p]).wait_send()
    by_rank = moved(2, (nz, nx, nc), back=True)

    z_all(5, sz).wait_recv()
    sp[mine] = jnp.sum(sz[...], axis=0)

    def p_copy(src, dst, peer):
        return pltpu.make_async_remote_copy(
            src_ref=src, dst_ref=dst, send_sem=psend.at[0], recv_sem=precv.at[0],
            device_id=peer, device_id_type=MESH,
        )

    for peer in around:
        p_copy(sp.at[mine], sp.at[mine], peer).start()

    z_all(4, ag).wait_recv()
    for k in range(nz):
        for h in range(halves):
            for j in range(pairs):
                first = 2 * (k * pairs + j)
                pt[h, first : first + 2] = ag[k, h * pairs + j].astype(f32)
    for h in range(halves):
        ps[c, x, :, h * lanes : (h + 1) * lanes] = pt[h].astype(bf16)
    x_spread(3, ps)
    z_all(4, ag).wait_send()
    z_all(5, sz).wait_send()

    bulk_onward((4, 5))
    x_arrived(2, oslab)
    for k, decay in enumerate((first_decay, second_decay)):
        old = oslab[:, :, k * r2 : (k + 1) * r2].reshape(rank, w)
        mold[k] = (decay * mul_t(old, by_rank)).reshape(nc, nx, share, rank)
    x_arrived(4, mslab)
    mnat[...] = mul(by_latent, mslab[...].reshape(latent, w)).astype(bf16)
    for copy in bulk:
        copy.wait_send()
    for dx in range(nx):
        c_bulk(oslab, dx, xp[dx]).wait_send()
        c_bulk(mslab, dx, xp[dx]).wait_send()

    everyone = sp.at[pl.ds(0, plane - 1)]
    p_copy(everyone, everyone, around[0]).wait_recv()
    p_copy(everyone, everyone, around[0]).wait_send()

    mean = jnp.sum(sp[...], axis=0)[:, 0:1] / count + mean_guard
    scale = 1.0 / jnp.sqrt(mean)
    scale_out[...] = jnp.broadcast_to(scale, scale_out.shape)

    def settle(core, p):
        scaled = ps[core, p].astype(f32) * scale
        first_new = mold[0, core, p] + (1.0 - first_decay) * scaled
        second_new = mold[1, core, p] + (1.0 - second_decay) * scaled * scaled
        heads[core, p] = (first_new / (jnp.sqrt(second_new) + root_guard)).astype(bf16)

    settle(c, x)
    for dx in X_ORDER[nx][::-1]:
        p = lax.rem(x + dx, nx)
        x_from(3, ps.at[c, p], dx)
        c_copy(3, dx, ps.at[c, p], ps.at[c, p]).start()
    for dx in X_ORDER[nx][::-1]:
        settle(c, lax.rem(x + dx, nx))
    for dx in (0,) + X_ORDER[nx][::-1]:
        p = lax.rem(x + dx, nx)
        c_copy(3, dx, ps.at[other, p], ps.at[other, p]).wait_recv()
        settle(other, p)
    x_left(3, ps)


def moments(scaled, first_old, second_old):
    first = first_decay * first_old + (1.0 - first_decay) * scaled
    second = second_decay * second_old + (1.0 - second_decay) * scaled * scaled
    return first, second


def finish(sizes, *refs):
    (
        heads, proj, basis, master, scale, qb, qf, qs, kb, kf, ks,
        qf_out, qs_out, qstep_out, qcopy_out, kf_out, ks_out, kstep_out, kcopy_out,
        fresh_q, fresh_k, first_q, second_q, step_q, first_k, second_k, step_k, sems,
    ) = refs
    nz, nx, nc, nt = sizes
    rank = qb.shape[1]
    qw = qf.shape[1]
    z, x, c, _ = (lax.axis_index(a) for a in AXES)
    q_dir = heads[:qw]
    k_dir = heads[qw:]
    latent = basis.shape[0]
    cut = latent // 2
    copies = []

    def send(src, dst):
        copies.append(pltpu.make_async_copy(src, dst, sems.at[len(copies)]))
        copies[-1].start()

    def renew(columns, towards, old, fresh, out):
        for k in range(2):
            some = slice(k * cut, (k + 1) * cut)
            step = mul_by_t(basis[some, columns], towards)
            fresh[some] = (master[some, old].astype(f32) - step_size * step).astype(bf16)
            send(fresh.at[some], out.at[some])

    renew(slice(0, rank), q_dir, slice(0, qw), fresh_q, qcopy_out)
    own = 2 * ((z * nx + x) * nc + c) + lax.broadcasted_iota(jnp.int32, (8, rank), 0)
    mine = jnp.where(own == lax.broadcasted_iota(jnp.int32, (8, rank), 1), 1.0, 0.0).astype(bf16)
    scaled = mul_by_t(mine, proj[...])[:2] * scale[:, 0:1]
    first_q[...], second_q[...] = moments(scaled[:, :qw], qf[...], qs[...])
    first_k[...], second_k[...] = moments(scaled[:, qw:], kf[...], ks[...])
    step_q[...] = mul_by_t(qb[...], q_dir)
    step_k[...] = mul_by_t(kb[...], k_dir)
    for src, dst in (
        (first_q, qf_out), (second_q, qs_out), (step_q, qstep_out),
        (first_k, kf_out), (second_k, ks_out), (step_k, kstep_out),
    ):
        send(src, dst)
    renew(slice(rank, 2 * rank), k_dir, slice(qw, master.shape[1]), fresh_k, kcopy_out)
    for copy in copies:
        copy.wait()


X_ORDER = {2: (1,), 4: (2, 1, 3)}


def body(sizes, *args):
    nz, nx, nc, nt = sizes
    args = [pltpu.with_memory_space_constraint(a, pltpu.HBM) for a in args]
    ql, qg, qm, qb, qf, qs, kl, kg, km, kb, kf, ks = args
    qw, kw = qg.shape[1], kg.shape[1]
    w = qw + kw
    fs = nz * nx * nc
    lr, rank = qb.shape
    latent = lr * fs
    count = float(rank * w * nt)
    plane = nx * nc * nt
    share = w // (nc * nx)
    lanes = min(128, rank)
    pieces = (nz, rank // lanes * (share // nz // 2), 2, lanes)
    vmem = pl.BlockSpec(memory_space=pltpu.VMEM)
    hbm = pl.BlockSpec(memory_space=pltpu.HBM)
    shape = jax.ShapeDtypeStruct
    heads, proj, basis, master, scale, *small = pl.pallas_call(
        functools.partial(kernel, sizes, (qw, kw), count),
        out_shape=(
            shape((nc, nx, share, rank), bf16), shape((nc, nx, share, rank), bf16),
            shape((latent, 2 * rank), bf16), shape((latent, w), bf16), shape((1, 128), f32),
            *(shape(a.shape, a.dtype) for a in (qb, qf, qs, kb, kf, ks)),
        ),
        in_specs=[hbm] * 12,
        out_specs=[vmem] * 11,
        scratch_shapes=[
            pltpu.VMEM(ql.shape, bf16), pltpu.VMEM(qg.shape, bf16),
            pltpu.VMEM(kl.shape, bf16), pltpu.VMEM(kg.shape, bf16),
            *(pltpu.VMEM(a.shape, f32) for a in (qm, km)),
            pltpu.VMEM((nz, lr, 2 * rank), bf16),
            pltpu.VMEM((4, nz // 4, 8, w), bf16),
            pltpu.VMEM((nc, nx, nz * lr, 2 * rank), bf16),
            pltpu.VMEM((nc, nx, nz * 4, w), bf16),
            pltpu.VMEM((nc, nx, nz * lr, w), bf16),
            pltpu.VMEM((w, latent), f32),
            pltpu.VMEM((w, latent), bf16),
            pltpu.VMEM((nz * lr, 2 * rank), f32),
            pltpu.VMEM((nz * lr, w), f32),
            pltpu.VMEM((2, nc, nx, share, rank), f32),
            pltpu.VMEM((nx, share, latent), bf16),
            pltpu.VMEM((nx, share, latent), bf16),
            pltpu.VMEM((2, share, latent), bf16),
            pltpu.VMEM((2, share // 2, latent), bf16),
            pltpu.VMEM((nc, 2 * share, latent // nc), bf16),
            pltpu.VMEM((rank // lanes, share, lanes), f32),
            pltpu.VMEM(pieces, bf16),
            pltpu.VMEM(pieces, bf16),
            pltpu.VMEM(pieces, bf16),
            pltpu.VMEM((plane, 1, 128), f32),
            pltpu.VMEM((nz, 1, 128), f32),
            pltpu.SemaphoreType.DMA((14,)),
            pltpu.SemaphoreType.DMA((6,)), pltpu.SemaphoreType.DMA((6,)),
            pltpu.SemaphoreType.DMA((1,)), pltpu.SemaphoreType.DMA((1,)),
            pltpu.SemaphoreType.DMA((2, nx)), pltpu.SemaphoreType.DMA((2, nx)),
            pltpu.SemaphoreType.DMA((5, nx)), pltpu.SemaphoreType.DMA((5, nx)),
            pltpu.SemaphoreType.DMA((6,)), pltpu.SemaphoreType.DMA((6,)),
            pltpu.SemaphoreType.DMA((6,)), pltpu.SemaphoreType.DMA((6,)),
        ],
        compiler_params=pltpu.CompilerParams(
            collective_id=0, has_side_effects=True, vmem_limit_bytes=36 * 1024 * 1024
        ),
    )(*args)
    return pl.pallas_call(
        functools.partial(finish, sizes),
        out_shape=(
            shape(qf.shape, f32), shape(qs.shape, f32), shape(qm.shape, f32), shape((latent, qw), bf16),
            shape(kf.shape, f32), shape(ks.shape, f32), shape(km.shape, f32), shape((latent, kw), bf16),
        ),
        in_specs=[vmem] * 11,
        out_specs=[hbm] * 8,
        scratch_shapes=[
            pltpu.VMEM((latent, qw), bf16), pltpu.VMEM((latent, kw), bf16),
            *(pltpu.VMEM(a.shape, f32) for a in (qf, qs, qm, kf, ks, km)),
            pltpu.SemaphoreType.DMA((10,)),
        ],
        compiler_params=pltpu.CompilerParams(vmem_limit_bytes=20 * 1024 * 1024),
    )(heads.reshape(w, rank), proj.reshape(w, rank), basis, master, scale, *small)


def solution(mesh, chips=(16, 4, 2)):
    nt = mesh.shape["tp"]
    finer = Mesh(mesh.devices.reshape(*chips, nt), AXES)
    in_specs = (P(FS, None), P(FS, "t"), P(FS, "t"), P(FS, None), P(FS, "t"), P(FS, "t")) * 2
    out_specs = (P(FS, "t"), P(FS, "t"), P(FS, "t"), P(None, "t")) * 2
    return jax.shard_map(
        functools.partial(body, (*chips, nt)), mesh=finer, in_specs=in_specs, out_specs=out_specs, check_vma=False
    )
```

```python
import functools

import jax
import jax.numpy as jnp
from jax import lax
from jax.experimental import pallas as pl
from jax.experimental.pallas import tpu as pltpu
from jax.sharding import Mesh
from jax.sharding import PartitionSpec as P

AXES = ("z", "x", "c", "t")
FS = ("z", "x", "c")
MESH = pl.DeviceIdType.MESH
f32 = jnp.float32
bf16 = jnp.bfloat16

first_decay = 0.8
second_decay = 0.9
step_size = 0.5
mean_guard = 1e-06
root_guard = 1e-08


def log2(n):
    return n.bit_length() - 1


def part(v, low, size):
    return lax.shift_right_logical(v, low) & (size - 1)


def moved(rows, sizes, back=False):
    nz, nx, nc = sizes
    n = nz * nx * nc * rows
    lr, lz, lx, lc = log2(rows), log2(nz), log2(nx), log2(nc)
    nat = lax.broadcasted_iota(jnp.int32, (n, n), int(back))
    got = lax.broadcasted_iota(jnp.int32, (n, n), 1 - int(back))
    r = part(got, 0, rows)
    z = part(got, lr, nz)
    x = part(got, lr + lz, nx)
    c = part(got, lr + lz + lx, nc)
    want = ((z * nx + x) * nc + c) * rows + r
    return jnp.where(nat == want, 1.0, 0.0).astype(bf16)


def mul(a, b):
    return jnp.dot(a, b, preferred_element_type=f32)


def mul_by_t(a, b):
    return lax.dot_general(a, b, (((1,), (1,)), ((), ())), preferred_element_type=f32)


def mul_t(a, b):
    return lax.dot_general(a, b, (((0,), (0,)), ((), ())), preferred_element_type=f32)


def kernel(sizes, widths, count, *refs):
    nz, nx, nc, nt = sizes
    qw, kw = widths
    (
        ql, qg, qm_h, qb, qf_h, qs_h, kl, kg, km_h, kb, kf_h, ks_h,
        heads, ps, bnat, mnat, scale_out, qb_v, qf, qs, kb_v, kf, ks,
        ql_v, qg_v, kl_v, kg_v, qm, km,
        bz, mm, bslab, oslab, mslab, tokens, rounded, wide, wider, mold,
        rc, xs, rx, relay, hilo, pt, zs, rz, ag, sp, sz,
        load_sem, zsend, zrecv, psend, precv, xsend, xrecv, csend, crecv, rsend, rrecv, bsend, brecv,
    ) = refs
    w = qw + kw
    rank = qb.shape[1]
    lr = bz.shape[1]
    latent = lr * nz * nx * nc
    share = w // (nc * nx)
    lanes = pt.shape[2]
    halves = rank // lanes
    pairs = share // nz // 2
    z, x, c, t = (lax.axis_index(a) for a in AXES)
    other = 1 - c

    loads = [
        pltpu.make_async_copy(src, dst, load_sem.at[k])
        for k, (src, dst) in enumerate((
            (ql, ql_v), (qg, qg_v), (kl, kl_v), (kg, kg_v),
            (qb, bz.at[z, :, :rank]), (kb, bz.at[z, :, rank:]),
            (qf_h, qf), (qs_h, qs), (kf_h, kf), (ks_h, ks), (qm_h, qm), (km_h, km),
            (qb, qb_v), (kb, kb_v),
        ))
    ]

    barrier = pltpu.get_barrier_semaphore()
    plane = nx * nc * nt
    mine = (x * nc + c) * nt + t

    along = [nz // 2] + [nz // 2 + h * side for h in range(1, nz // 2) for side in (1, -1)]
    peers = [lax.rem(z + d, nz) for d in along]
    xp = [lax.rem(x + d, nx) for d in range(nx)]
    tp = [lax.rem(t + d, nt) for d in range(nt)]
    around = [
        (z, xp[dx], core, tp[dt])
        for dx in range(nx) for dt in range(nt) for core in (c, other)
        if dx or dt or core is other
    ]

    for p in peers:
        pl.semaphore_signal(barrier, inc=1, device_id=(p, x, c, t), device_id_type=MESH)
    for load in loads:
        load.start()
    for peer in around:
        pl.semaphore_signal(barrier, inc=1, device_id=peer, device_id_type=MESH)

    def z_copy(stage, src, dst, peer):
        return pltpu.make_async_remote_copy(
            src_ref=src, dst_ref=dst, send_sem=zsend.at[stage], recv_sem=zrecv.at[stage],
            device_id=(peer, x, c, t), device_id_type=MESH,
        )

    def z_spread(stage, buf):
        for p in peers:
            z_copy(stage, buf.at[z], buf.at[z], p).start()

    def z_all(stage, buf, n=nz - 1):
        return z_copy(stage, buf.at[pl.ds(0, n)], buf.at[pl.ds(0, n)], peers[0])

    def x_copy(stage, src, dst, dx):
        p = lax.rem(x + dx, nx)
        return pltpu.make_async_remote_copy(
            src_ref=src, dst_ref=dst,
            send_sem=xsend.at[stage // 3, dx], recv_sem=xrecv.at[stage // 3, nx - dx],
            device_id=(z, p, c, t), device_id_type=MESH,
        )

    def x_from(stage, buf, dx):
        pltpu.make_async_remote_copy(
            src_ref=buf, dst_ref=buf,
            send_sem=xsend.at[stage // 3, dx], recv_sem=xrecv.at[stage // 3, dx],
            device_id=(z, lax.rem(x + dx, nx), c, t), device_id_type=MESH,
        ).wait_recv()

    right, across, left = xp[1], xp[2], xp[3]
    half = share // 2
    ahead, behind = pl.ds(0, half), pl.ds(half, half)

    def beside(sends, recvs, k, rightward, src, dst):
        return pltpu.make_async_remote_copy(
            src_ref=src, dst_ref=dst, send_sem=sends.at[k], recv_sem=recvs.at[k],
            device_id=(z, right if rightward else left, c, t), device_id_type=MESH,
        )

    def c_copy(stage, k, src, dst):
        return pltpu.make_async_remote_copy(
            src_ref=src, dst_ref=dst,
            send_sem=csend.at[stage, k], recv_sem=crecv.at[stage, k],
            device_id=(z, x, other, t), device_id_type=MESH,
        )

    def x_spread(stage, slabs):
        for dx in X_ORDER[nx]:
            x_copy(stage, slabs.at[c, x], slabs.at[c, x], dx).start()
        c_copy(stage, 0, slabs.at[c, x], slabs.at[c, x]).start()

    def x_onward(stage, slabs):
        for dx in X_ORDER[nx][::-1]:
            p = lax.rem(x + dx, nx)
            x_from(stage, slabs.at[c, p], dx)
            c_copy(stage, dx, slabs.at[c, p], slabs.at[c, p]).start()

    def x_arrived(stage, slabs):
        for dx in range(nx):
            p = lax.rem(x + dx, nx)
            c_copy(stage, dx, slabs.at[other, p], slabs.at[other, p]).wait_recv()

    def x_left(stage, slabs):
        for dx in range(1, nx):
            x_copy(stage, slabs.at[c, x], slabs.at[c, x], dx).wait_send()
        for dx in range(nx):
            p = lax.rem(x + dx, nx)
            c_copy(stage, dx, slabs.at[c, p], slabs.at[c, p]).wait_send()

    def rows(core, p):
        return pl.ds(pl.multiple_of((core * nx + p) * share, share), share)

    for load in loads[:2]:
        load.wait()
    tokens[:qw] = mul_t(qg_v[...], ql_v[...])
    for load in loads[2:4]:
        load.wait()
    tokens[qw:] = mul_t(kg_v[...], kl_v[...])
    rounded[...] = tokens[...].astype(bf16)
    for load in loads[4:]:
        load.wait()
    zr, zq = lax.rem(z, 4), z // 4
    mm[zr, zq, 0:2, :qw] = qf[...].astype(bf16)
    mm[zr, zq, 0:2, qw:] = kf[...].astype(bf16)
    mm[zr, zq, 2:4, :qw] = qs[...].astype(bf16)
    mm[zr, zq, 2:4, qw:] = ks[...].astype(bf16)
    mm[zr, zq, 4:8, :qw] = qm[...].astype(bf16)
    mm[zr, zq, 4:8, qw:] = km[...].astype(bf16)
    pl.semaphore_wait(barrier, nz - 1 + plane - 1)

    order = X_ORDER[nx] + (0,)
    z_spread(0, bz)
    for dx in order:
        p = lax.rem(x + dx, nx)
        c_copy(1, dx, rounded.at[rows(other, p)], rc.at[p]).start()

    sums = (
        beside(rsend, rrecv, 0, True, xs.at[across, ahead], relay.at[0]),
        beside(rsend, rrecv, 1, False, xs.at[across, behind], relay.at[1]),
        beside(rsend, rrecv, 2, True, xs.at[right, behind], rx.at[0, behind]),
        beside(rsend, rrecv, 3, False, xs.at[left, ahead], rx.at[1, ahead]),
        beside(rsend, rrecv, 4, True, xs.at[right, ahead], rx.at[0, ahead]),
        beside(rsend, rrecv, 5, False, xs.at[left, behind], rx.at[1, behind]),
    )
    for dx in order:
        p = xp[dx]
        c_copy(1, dx, rc.at[p], rc.at[p]).wait_recv()
        both = tokens[rows(c, p)] + rc[p].astype(f32)
        if dx == 2:
            xs[p] = both.astype(bf16)
            sums[0].start()
            sums[1].start()
        elif dx == 1:
            xs[p, half:] = both[half:].astype(bf16)
            sums[2].start()
            tokens[rows(c, p)] = both
        elif dx == 3:
            xs[p, :half] = both[:half].astype(bf16)
            sums[3].start()
            tokens[rows(c, p)] = both
        else:
            tokens[rows(c, p)] = both

    for k in range(1, nz // 4):
        z_copy(1, mm.at[zr, zq], mm.at[zr, zq], lax.rem(z + 4 * k, nz)).start()
    by_latent = moved(lr, (nz, nx, nc))

    sums[0].wait_recv()
    passed = tokens[rows(c, right)]
    xs[right, :half] = (passed[:half] + relay[0].astype(f32)).astype(bf16)
    sums[4].start()
    sums[1].wait_recv()
    passed = tokens[rows(c, left)]
    xs[left, half:] = (passed[half:] + relay[1].astype(f32)).astype(bf16)
    sums[5].start()

    z_all(0, bz).wait_recv()
    for k in range(nz):
        wide[lr * k : lr * (k + 1), :] = bz[k].astype(f32)
    bslab[c, x] = wide[...].astype(bf16)
    x_spread(0, bslab)

    total = tokens[rows(c, x)]
    for k in range(2, 6):
        sums[k].wait_recv()
    total = total + rx[0].astype(f32) + rx[1].astype(f32)
    high = total.astype(bf16)
    low = (total - high.astype(f32)).astype(bf16)
    part_of = latent // nc
    turned_high = mul(high, by_latent).astype(bf16)
    turned_low = mul(low, by_latent).astype(bf16)
    for k in range(nc):
        hilo[k, :share] = turned_high[:, k * part_of : (k + 1) * part_of]
        hilo[k, share:] = turned_low[:, k * part_of : (k + 1) * part_of]

    fours = nz // 4
    if fours > 1:
        z_all(1, mm.at[0], fours - 1).wait_recv()
    for d, some in (
        (2, pl.ds(0, (fours + 1) // 2)), (nz - 2, pl.ds((fours + 1) // 2, fours // 2)),
        (1, pl.ds(0, fours)), (nz - 1, pl.ds(0, fours)),
    ):
        if some.size:
            z_copy(2, mm.at[zr, some], mm.at[zr, some], lax.rem(z + d, nz)).start()

    x_onward(0, bslab)
    got = mul(hilo[c], bslab[c].reshape(part_of, 2 * rank))
    x_arrived(0, bslab)
    got = got + mul(hilo[other], bslab[other].reshape(part_of, 2 * rank))
    got = got[:share] + got[share:]
    column = (c * nx + x) * share + lax.broadcasted_iota(jnp.int32, (share, rank), 0)
    got = jnp.where(column < qw, got[:, :rank], got[:, rank:])
    for h in range(halves):
        pt[h] = got[:, h * lanes : (h + 1) * lanes]
    for k in range(nz):
        for h in range(halves):
            for j in range(pairs):
                first = 2 * (k * pairs + j)
                zs[k, h * pairs + j] = pt[h, first : first + 2].astype(bf16)

    for p in peers:
        z_copy(3, zs.at[p], rz.at[z], p).start()
    rz[z] = zs[z]

    z_all(2, mm, 3).wait_recv()
    r2 = 2 * nz
    for k in range(nz):
        wider[2 * k : 2 * k + 2, :] = mm[k % 4, k // 4, 0:2].astype(f32)
        wider[r2 + 2 * k : r2 + 2 * k + 2, :] = mm[k % 4, k // 4, 2:4].astype(f32)
    oslab[c, x] = wider[...].astype(bf16)
    for k in range(nz):
        wider[lr * k : lr * (k + 1), :] = mm[k % 4, k // 4, 4:8].astype(f32)
    mslab[c, x] = wider[...].astype(bf16)
    bulk = (
        beside(bsend, brecv, 0, True, oslab.at[c, x], oslab.at[c, x]),
        beside(bsend, brecv, 1, False, mslab.at[c, x], mslab.at[c, x]),
        beside(bsend, brecv, 2, True, mslab.at[c, x], mslab.at[c, x]),
        beside(bsend, brecv, 3, False, oslab.at[c, x], oslab.at[c, x]),
        beside(bsend, brecv, 4, True, oslab.at[c, left], oslab.at[c, left]),
        beside(bsend, brecv, 5, False, mslab.at[c, right], mslab.at[c, right]),
    )
    landing = (
        (0, True, oslab, left, 3), (1, False, mslab, right, 1), (2, True, mslab, left, 3),
        (3, False, oslab, right, 1), (4, True, oslab, across, 2), (5, False, mslab, across, 2),
    )

    def c_bulk(slabs, dx, p):
        return c_copy(2 if slabs is oslab else 4, dx, slabs.at[c, p], slabs.at[c, p])

    def bulk_onward(which):
        for k in which:
            _, rightward, slabs, p, dx = landing[k]
            beside(bsend, brecv, k, rightward, slabs.at[c, p], slabs.at[c, p]).wait_recv()
            if k < 2:
                bulk[4 + k].start()
            c_bulk(slabs, dx, p).start()

    for copy in bulk[:4]:
        copy.start()
    c_bulk(oslab, 0, x).start()
    c_bulk(mslab, 0, x).start()
    z_all(0, bz).wait_send()
    if nz > 4:
        z_all(1, mm.at[0], nz // 4 - 1).wait_send()
    z_all(2, mm, 3).wait_send()
    bnat[...] = mul(by_latent, bslab[...].reshape(latent, 2 * rank)).astype(bf16)

    z_all(3, rz).wait_recv()
    proj = rz[0].astype(f32)
    for k in range(1, nz):
        proj = proj + rz[k].astype(f32)
    ag[z] = proj.astype(bf16)
    z_spread(4, ag)

    def p_copy(src, dst, peer):
        return pltpu.make_async_remote_copy(
            src_ref=src, dst_ref=dst, send_sem=psend.at[0], recv_sem=precv.at[0],
            device_id=peer, device_id_type=MESH,
        )

    sp[mine] = jnp.full((1, 128), jnp.sum(proj * proj), f32)
    for peer in around:
        p_copy(sp.at[mine], sp.at[mine], peer).start()
    everyone = sp.at[pl.ds(0, plane - 1)]

    bulk_onward((0, 1))
    p_copy(everyone, everyone, around[0]).wait_recv()
    sz[z] = jnp.sum(sp[...], axis=0)
    z_spread(5, sz)
    bulk_onward((2, 3))
    z_all(3, zs).wait_send()
    x_left(0, bslab)
    for copy in sums:
        copy.wait_send()
    for dx in range(nx):
        p = xp[dx]
        c_copy(1, dx, rounded.at[rows(other, p)], rc.at[p]).wait_send()
    by_rank = moved(2, (nz, nx, nc), back=True)

    z_all(4, ag).wait_recv()
    for k in range(nz):
        for h in range(halves):
            for j in range(pairs):
                first = 2 * (k * pairs + j)
                pt[h, first : first + 2] = ag[k, h * pairs + j].astype(f32)
    for h in range(halves):
        ps[c, x, :, h * lanes : (h + 1) * lanes] = pt[h].astype(bf16)
    x_spread(3, ps)
    z_all(4, ag).wait_send()

    bulk_onward((4, 5))
    x_arrived(2, oslab)
    for k, decay in enumerate((first_decay, second_decay)):
        old = oslab[:, :, k * r2 : (k + 1) * r2].reshape(rank, w)
        mold[k] = (decay * mul_t(old, by_rank)).reshape(nc, nx, share, rank)
    x_arrived(4, mslab)
    mnat[...] = mul(by_latent, mslab[...].reshape(latent, w)).astype(bf16)
    for copy in bulk:
        copy.wait_send()
    for dx in range(nx):
        c_bulk(oslab, dx, xp[dx]).wait_send()
        c_bulk(mslab, dx, xp[dx]).wait_send()

    p_copy(everyone, everyone, around[0]).wait_send()
    for dx in X_ORDER[nx][::-1]:
        p = lax.rem(x + dx, nx)
        x_from(3, ps.at[c, p], dx)
        c_copy(3, dx, ps.at[c, p], ps.at[c, p]).start()
    z_all(5, sz).wait_send()
    z_all(5, sz).wait_recv()

    mean = jnp.sum(sz[...], axis=0)[:, 0:1] / count + mean_guard
    scale = 1.0 / jnp.sqrt(mean)
    scale_out[...] = jnp.broadcast_to(scale, scale_out.shape)

    def settle(core, p):
        scaled = ps[core, p].astype(f32) * scale
        first_new = mold[0, core, p] + (1.0 - first_decay) * scaled
        second_new = mold[1, core, p] + (1.0 - second_decay) * scaled * scaled
        heads[core, p] = (first_new / (jnp.sqrt(second_new) + root_guard)).astype(bf16)

    settle(c, x)
    for dx in X_ORDER[nx][::-1]:
        settle(c, lax.rem(x + dx, nx))
    for dx in (0,) + X_ORDER[nx][::-1]:
        p = lax.rem(x + dx, nx)
        c_copy(3, dx, ps.at[other, p], ps.at[other, p]).wait_recv()
        settle(other, p)
    x_left(3, ps)


def moments(scaled, first_old, second_old):
    first = first_decay * first_old + (1.0 - first_decay) * scaled
    second = second_decay * second_old + (1.0 - second_decay) * scaled * scaled
    return first, second


def finish(sizes, *refs):
    (
        heads, proj, basis, master, scale, qb, qf, qs, kb, kf, ks,
        qf_out, qs_out, qstep_out, qcopy_out, kf_out, ks_out, kstep_out, kcopy_out,
        fresh_q, fresh_k, first_q, second_q, step_q, first_k, second_k, step_k, sems,
    ) = refs
    nz, nx, nc, nt = sizes
    rank = qb.shape[1]
    qw = qf.shape[1]
    z, x, c, _ = (lax.axis_index(a) for a in AXES)
    q_dir = heads[:qw]
    k_dir = heads[qw:]
    latent = basis.shape[0]
    cut = latent // 2
    copies = []

    def send(src, dst):
        copies.append(pltpu.make_async_copy(src, dst, sems.at[len(copies)]))
        copies[-1].start()

    def renew(columns, towards, old, fresh, out):
        for k in range(2):
            some = slice(k * cut, (k + 1) * cut)
            step = mul_by_t(basis[some, columns], towards)
            fresh[some] = (master[some, old].astype(f32) - step_size * step).astype(bf16)
            send(fresh.at[some], out.at[some])

    renew(slice(0, rank), q_dir, slice(0, qw), fresh_q, qcopy_out)
    own = 2 * ((z * nx + x) * nc + c) + lax.broadcasted_iota(jnp.int32, (8, rank), 0)
    mine = jnp.where(own == lax.broadcasted_iota(jnp.int32, (8, rank), 1), 1.0, 0.0).astype(bf16)
    scaled = mul_by_t(mine, proj[...])[:2] * scale[:, 0:1]
    first_q[...], second_q[...] = moments(scaled[:, :qw], qf[...], qs[...])
    first_k[...], second_k[...] = moments(scaled[:, qw:], kf[...], ks[...])
    step_q[...] = mul_by_t(qb[...], q_dir)
    step_k[...] = mul_by_t(kb[...], k_dir)
    for src, dst in (
        (first_q, qf_out), (second_q, qs_out), (step_q, qstep_out),
        (first_k, kf_out), (second_k, ks_out), (step_k, kstep_out),
    ):
        send(src, dst)
    renew(slice(rank, 2 * rank), k_dir, slice(qw, master.shape[1]), fresh_k, kcopy_out)
    for copy in copies:
        copy.wait()


X_ORDER = {2: (1,), 4: (2, 1, 3)}


def body(sizes, *args):
    nz, nx, nc, nt = sizes
    args = [pltpu.with_memory_space_constraint(a, pltpu.HBM) for a in args]
    ql, qg, qm, qb, qf, qs, kl, kg, km, kb, kf, ks = args
    qw, kw = qg.shape[1], kg.shape[1]
    w = qw + kw
    fs = nz * nx * nc
    lr, rank = qb.shape
    latent = lr * fs
    count = float(rank * w * nt)
    plane = nx * nc * nt
    share = w // (nc * nx)
    lanes = min(128, rank)
    pieces = (nz, rank // lanes * (share // nz // 2), 2, lanes)
    vmem = pl.BlockSpec(memory_space=pltpu.VMEM)
    hbm = pl.BlockSpec(memory_space=pltpu.HBM)
    shape = jax.ShapeDtypeStruct
    heads, proj, basis, master, scale, *small = pl.pallas_call(
        functools.partial(kernel, sizes, (qw, kw), count),
        out_shape=(
            shape((nc, nx, share, rank), bf16), shape((nc, nx, share, rank), bf16),
            shape((latent, 2 * rank), bf16), shape((latent, w), bf16), shape((1, 128), f32),
            *(shape(a.shape, a.dtype) for a in (qb, qf, qs, kb, kf, ks)),
        ),
        in_specs=[hbm] * 12,
        out_specs=[vmem] * 11,
        scratch_shapes=[
            pltpu.VMEM(ql.shape, bf16), pltpu.VMEM(qg.shape, bf16),
            pltpu.VMEM(kl.shape, bf16), pltpu.VMEM(kg.shape, bf16),
            *(pltpu.VMEM(a.shape, f32) for a in (qm, km)),
            pltpu.VMEM((nz, lr, 2 * rank), bf16),
            pltpu.VMEM((4, nz // 4, 8, w), bf16),
            pltpu.VMEM((nc, nx, nz * lr, 2 * rank), bf16),
            pltpu.VMEM((nc, nx, nz * 4, w), bf16),
            pltpu.VMEM((nc, nx, nz * lr, w), bf16),
            pltpu.VMEM((w, latent), f32),
            pltpu.VMEM((w, latent), bf16),
            pltpu.VMEM((nz * lr, 2 * rank), f32),
            pltpu.VMEM((nz * lr, w), f32),
            pltpu.VMEM((2, nc, nx, share, rank), f32),
            pltpu.VMEM((nx, share, latent), bf16),
            pltpu.VMEM((nx, share, latent), bf16),
            pltpu.VMEM((2, share, latent), bf16),
            pltpu.VMEM((2, share // 2, latent), bf16),
            pltpu.VMEM((nc, 2 * share, latent // nc), bf16),
            pltpu.VMEM((rank // lanes, share, lanes), f32),
            pltpu.VMEM(pieces, bf16),
            pltpu.VMEM(pieces, bf16),
            pltpu.VMEM(pieces, bf16),
            pltpu.VMEM((plane, 1, 128), f32),
            pltpu.VMEM((nz, 1, 128), f32),
            pltpu.SemaphoreType.DMA((14,)),
            pltpu.SemaphoreType.DMA((6,)), pltpu.SemaphoreType.DMA((6,)),
            pltpu.SemaphoreType.DMA((1,)), pltpu.SemaphoreType.DMA((1,)),
            pltpu.SemaphoreType.DMA((2, nx)), pltpu.SemaphoreType.DMA((2, nx)),
            pltpu.SemaphoreType.DMA((5, nx)), pltpu.SemaphoreType.DMA((5, nx)),
            pltpu.SemaphoreType.DMA((6,)), pltpu.SemaphoreType.DMA((6,)),
            pltpu.SemaphoreType.DMA((6,)), pltpu.SemaphoreType.DMA((6,)),
        ],
        compiler_params=pltpu.CompilerParams(
            collective_id=0, has_side_effects=True, vmem_limit_bytes=36 * 1024 * 1024
        ),
    )(*args)
    return pl.pallas_call(
        functools.partial(finish, sizes),
        out_shape=(
            shape(qf.shape, f32), shape(qs.shape, f32), shape(qm.shape, f32), shape((latent, qw), bf16),
            shape(kf.shape, f32), shape(ks.shape, f32), shape(km.shape, f32), shape((latent, kw), bf16),
        ),
        in_specs=[vmem] * 11,
        out_specs=[hbm] * 8,
        scratch_shapes=[
            pltpu.VMEM((latent, qw), bf16), pltpu.VMEM((latent, kw), bf16),
            *(pltpu.VMEM(a.shape, f32) for a in (qf, qs, qm, kf, ks, km)),
            pltpu.SemaphoreType.DMA((10,)),
        ],
        compiler_params=pltpu.CompilerParams(vmem_limit_bytes=20 * 1024 * 1024),
    )(heads.reshape(w, rank), proj.reshape(w, rank), basis, master, scale, *small)


def solution(mesh, chips=(16, 4, 2)):
    nt = mesh.shape["tp"]
    finer = Mesh(mesh.devices.reshape(*chips, nt), AXES)
    in_specs = (P(FS, None), P(FS, "t"), P(FS, "t"), P(FS, None), P(FS, "t"), P(FS, "t")) * 2
    out_specs = (P(FS, "t"), P(FS, "t"), P(FS, "t"), P(None, "t")) * 2
    return jax.shard_map(
        functools.partial(body, (*chips, nt)), mesh=finer, in_specs=in_specs, out_specs=out_specs, check_vma=False
    )
```
